32 devices in a mesh: grp: 2 (over y), sp: 4 (over z), tp: 2 (over x), dp: 2 (over core).
Axes of the slice: x: 2, y: 2, z: 4, core: 2. Of those that a mesh axis runs over, the one named last changes fastest.
Arguments:
- latent: bfloat16 [6144, 4096], P(('grp', 'sp', 'dp')), parts along dimension 0, may hold values from -6 to 6
- context: bfloat16 [1024, 4096], P(('grp', 'sp')), parts along dimension 0, may hold values from -6 to 6
- condition: bfloat16 [8192], P('grp'), parts along dimension 0, may hold values from -6 to 6
- context_condition: bfloat16 [4096], replicated, may hold values from -6 to 6
- shift_weight: bfloat16 [4096, 4096], P('sp', ('tp', 'dp')), may hold values from -0.09375 to 0.09375
- scale_weight: bfloat16 [4096, 4096], P('sp', ('tp', 'dp')), may hold values from -0.09375 to 0.09375
- gate_weight: bfloat16 [4096, 4096], P('sp', ('tp', 'dp')), may hold values from -0.09375 to 0.09375
- norm_gain: float32 [4096], replicated, may hold values from 0.1 to 1.9
- out_gate_weight: bfloat16 [4096, 2048], P(None, ('tp', 'dp')), may hold values from -0.09375 to 0.09375
- signal_weight: bfloat16 [4096, 2048], P(None, ('tp', 'dp')), may hold values from -0.09375 to 0.09375
- writer_weight: bfloat16 [4096, 1024], P(None, ('tp', 'dp')), may hold values from -0.09375 to 0.09375
- reader_matrix: bfloat16 [4096, 1024], P(None, ('tp', 'dp')), may hold values from -0.09375 to 0.09375
- step_weight: bfloat16 [2, 4096, 32], P(None, None, ('tp', 'dp')), may hold values from -0.09375 to 0.09375
- signal_taps: float32 [3, 2048], P(None, ('tp', 'dp')), may hold values from -3.5 to 3.5
- writer_taps: float32 [3, 1024], P(None, ('tp', 'dp')), may hold values from -3.5 to 3.5
- reader_taps: float32 [3, 1024], P(None, ('tp', 'dp')), may hold values from -3.5 to 3.5
- step_bias: float32 [2, 32], P(None, ('tp', 'dp')), may hold values from -4.5 to -2.5
- decay_log: float32 [2, 32], P(None, ('tp', 'dp')), may hold values from -12 to 1
- decay_extra: float32 [2, 32, 6144], P(None, ('tp', 'dp'), ('grp', 'sp')), parts along dimension 2, may hold values from -3 to 0
- group_gain: float32 [2048], P(('tp', 'dp')), may hold values from 0.1 to 1.9
- output_weight: bfloat16 [2048, 4096], P(None, ('tp', 'dp')), may hold values from -0.125 to 0.125
Outputs:
- updated: bfloat16 [6144, 4096], P(('grp', 'sp'), ('tp', 'dp')), parts along dimension 0
The draws below stay inside these ranges and needn't reach their ends.
There are 2 independent parts, one for each index of `grp`. The reference program is written for one: setup_inputs(seed, part) draws one part's arguments, and reference() takes and returns one part's arrays. A program takes and returns all parts, laid end to end along the dimension named above; an argument that names none is the same for every part. Nothing has to cross between parts.
All inputs are finite; a program needn't handle non-finite values.
Results may differ from the reference program's by a relative error of at most 0.007.
Values may be sent and summed in bfloat16 or wider, within the bound.
A program may use at most 128 MiB of HBM per device.

```python
import math
import jax
import jax.numpy as jnp
from jax import lax

D = 4096
HEADS = 32
HEAD_DIM = 64
GROUPS = 8
STATE = 128
W_INNER = 2048
BLOCK = 128
TAPS = 3
TOK_DEV = 768
TOKENS = 3072
CTX = 512


def draw_decay_log(key, part):
    first, second, third = jax.random.split(key, 3)
    chain_len = TOKENS + CTX
    slow = jax.random.uniform(first, (2, HEADS), jnp.float32, math.log(2.0 / chain_len), math.log(10.0 / chain_len))
    fast = jax.random.uniform(second, (2, HEADS), jnp.float32, math.log(0.5), math.log(2.0))
    picks = jax.random.randint(third, (2, HEADS), 0, 2)
    chosen = jnp.where(picks == 1, fast, slow)
    return chosen


def draw_decay_extra(key, part):
    first, second, third = jax.random.split(key, 3)
    span_count = TOKENS // TOK_DEV
    low_end, high_end = (0.1, 1.2)
    rate = jnp.exp(jax.random.uniform(first, (2, HEADS, span_count), jnp.float32, math.log(low_end), math.log(high_end))) / TOKENS
    equilibrium_memory = jnp.repeat(rate, TOK_DEV, axis=2)
    spots = jax.random.randint(second, (2, HEADS, 4), 0, TOKENS)
    stack_level_index = jax.random.uniform(third, (2, HEADS, 4), jnp.float32, math.log(0.5), math.log(0.8))
    places = lax.iota(jnp.int32, TOKENS)
    agreeing_tally = places[None, None, None, :] == spots[..., None]
    latent_block_tally = jnp.sum(jnp.where(agreeing_tally, stack_level_index[..., None], 0.0), axis=2)
    return latent_block_tally - equilibrium_memory


def level_of(rng, dims, shards, smallest, largest):
    factor_of, own = 1.0, jax.random.fold_in(rng, 6)
    for dim, blocks in shards:
        steps = jnp.exp(jax.random.uniform(jax.random.fold_in(own, dim), (blocks,), jnp.float32, smallest / len(shards), largest / len(shards)))
        factor_of = factor_of * jnp.repeat(steps, dims[dim] // blocks).reshape([-1 if axis == dim else 1 for axis in range(len(dims))])
    return factor_of


def bell_draw(stream_key, dims, spread, most, pieces=(), kind=jnp.bfloat16):
    level = level_of(stream_key, dims, pieces, -0.22, 0.18) if pieces else 1.0
    entries = jax.random.normal(stream_key, dims, jnp.float32) * spread * level
    return jnp.minimum(jnp.maximum(entries, -most), most).astype(kind)


def setup_inputs(seed: int = 0, part: int = 0) -> dict:
    arg_keys = jax.random.split(jax.random.key(seed), 22)
    part_splits = jax.random.split(jax.random.fold_in(arg_keys[21], part), 22)
    return {
        "latent": bell_draw(part_splits[0], (TOKENS, D), 1.0, 6.0, ((0, 8),)),
        "context": bell_draw(part_splits[1], (CTX, D), 1.0, 6.0, ((0, 4),)),
        "condition": bell_draw(part_splits[2], (D,), 1.0, 6.0),
        "context_condition": bell_draw(arg_keys[3], (D,), 1.0, 6.0),
        "shift_weight": bell_draw(arg_keys[4], (D, D), D ** -0.5, 0.09375, ((0, 4), (1, 4))),
        "scale_weight": bell_draw(arg_keys[5], (D, D), D ** -0.5, 0.09375, ((0, 4), (1, 4))),
        "gate_weight": bell_draw(arg_keys[6], (D, D), D ** -0.5, 0.09375, ((0, 4), (1, 4))),
        "norm_gain": jnp.clip(1.0 + 0.18 * jax.random.normal(arg_keys[7], (D,), jnp.float32), 0.1, 1.9),
        "out_gate_weight": bell_draw(arg_keys[8], (D, W_INNER), D ** -0.5, 0.09375, ((1, 4),)),
        "signal_weight": bell_draw(arg_keys[9], (D, W_INNER), D ** -0.5, 0.09375, ((1, 4),)),
        "writer_weight": bell_draw(arg_keys[10], (D, GROUPS * STATE), D ** -0.5, 0.09375, ((1, 4),)),
        "reader_matrix": bell_draw(arg_keys[11], (D, GROUPS * STATE), D ** -0.5, 0.09375, ((1, 4),)),
        "step_weight": bell_draw(arg_keys[12], (2, D, HEADS), D ** -0.5, 0.09375, ((2, 4),)),
        "signal_taps": bell_draw(arg_keys[13], (TAPS, W_INNER), TAPS ** -0.5, 3.5, ((1, 4),), jnp.float32),
        "writer_taps": bell_draw(arg_keys[14], (TAPS, GROUPS * STATE), TAPS ** -0.5, 3.5, ((1, 4),), jnp.float32),
        "reader_taps": bell_draw(arg_keys[15], (TAPS, GROUPS * STATE), TAPS ** -0.5, 3.5, ((1, 4),), jnp.float32),
        "step_bias": jnp.clip(-4.5 + 2.0 * jax.random.uniform(arg_keys[16], (2, HEADS), jnp.float32) ** level_of(arg_keys[16], (2, HEADS), ((1, 4),), -0.2, 0.2), -4.5, -2.5),
        "decay_log": draw_decay_log(jax.random.fold_in(arg_keys[21], 71), part),
        "decay_extra": draw_decay_extra(jax.random.fold_in(jax.random.fold_in(arg_keys[21], part), 71), part),
        "group_gain": jnp.clip(1.0 + 0.18 * jax.random.normal(arg_keys[19], (W_INNER,), jnp.float32), 0.1, 1.9),
        "output_weight": bell_draw(arg_keys[20], (W_INNER, D), W_INNER ** -0.5, 0.125, ((1, 4),)),
    }


EPSILON = 1e-06
HIGHEST = lax.Precision.HIGHEST

def modulate(rows, norm_gain, shift_vec, scale_vec):
    values = rows.astype(jnp.float32)
    normed = values * lax.rsqrt(lax.optimization_barrier(jnp.mean(values * values, axis=-1, keepdims=True)) + EPSILON) * norm_gain
    return (normed * (1.0 + scale_vec) + shift_vec).astype(jnp.bfloat16)

def centred_conv(padded, conv_taps, length):
    running = jnp.zeros((length, padded.shape[1]), jnp.float32)
    for offset in range(conv_taps.shape[0]):
        running = running + conv_taps[offset] * padded[offset:offset + length].astype(jnp.float32)
    return jax.nn.silu(running)

def project_rows(hidden, signal_weight, writer_weight, reader_matrix, step_weight):
    raw_cols = jnp.concatenate([jnp.dot(hidden, signal_weight, preferred_element_type=jnp.float32), jnp.dot(hidden, writer_weight, preferred_element_type=jnp.float32), jnp.dot(hidden, reader_matrix, preferred_element_type=jnp.float32)], axis=1).astype(jnp.bfloat16)
    step_in = jnp.stack([jnp.dot(hidden, step_weight[0], preferred_element_type=jnp.float32), jnp.dot(hidden, step_weight[1], preferred_element_type=jnp.float32)]).astype(jnp.bfloat16)
    return (raw_cols, step_in)

def split_mixed(conv_out, head_count, head_width, group_count, state_width):
    length = conv_out.shape[0]
    signal_end = head_count * head_width
    writer_end = signal_end + group_count * state_width
    signal = conv_out[:, :signal_end].reshape(length, head_count, head_width)
    writer = conv_out[:, signal_end:writer_end].reshape(length, group_count, state_width)
    reader = conv_out[:, writer_end:].reshape(length, group_count, state_width)
    return (signal, writer, reader)

def state_span(signal, step_size, log_decay, writer, reader, start_state, block):
    length, head_count, head_width = signal.shape
    group_count, state_width = (writer.shape[1], writer.shape[2])
    per_group = head_count // group_count
    blocks = length // block
    scaled = (signal * step_size[..., None]).reshape(blocks, block, group_count, per_group, head_width)
    cum_log = jnp.cumsum(log_decay.reshape(blocks, block, group_count, per_group), axis=1)
    writer_blk = writer.reshape(blocks, block, group_count, state_width)
    reader_blk = reader.reshape(blocks, block, group_count, state_width)
    inner_dot = jnp.einsum('bign,bjgn->bgij', reader_blk, writer_blk, precision=HIGHEST)
    moved = jnp.moveaxis(cum_log, 1, -1)
    gap_logs = moved[..., :, None] - moved[..., None, :]
    lower_mask = jnp.tril(jnp.ones((block, block), dtype=bool))
    weights = jnp.exp(jnp.where(lower_mask, gap_logs, -jnp.inf))
    in_block = jnp.einsum('bgij,bgeij,bjgep->bigep', inner_dot, weights, scaled, precision=HIGHEST)
    to_end = jnp.exp(cum_log[:, -1:] - cum_log)
    states = jnp.einsum('bjgn,bjge,bjgep->bgepn', writer_blk, to_end, scaled, precision=HIGHEST)
    block_decay = jnp.exp(cum_log[:, -1])

    def advance(running, block_item):
        state_add, decay_now = block_item
        return (running * decay_now[..., None, None] + state_add, running)
    last_state, before = lax.scan(advance, start_state.reshape(group_count, per_group, head_width, state_width), (states, block_decay))
    carried = jnp.einsum('bign,bgepn,bige->bigep', reader_blk, before, jnp.exp(cum_log), precision=HIGHEST)
    result = (in_block + carried).reshape(length, head_count, head_width)
    return (result, last_state.reshape(head_count, head_width, state_width))

def context_state(signal, row_weights, writer):
    length, head_count, head_width = signal.shape
    group_count, state_width = (writer.shape[1], writer.shape[2])
    per_group = head_count // group_count
    grouped = signal.reshape(length, group_count, per_group, head_width)
    weights = row_weights.reshape(length, group_count, per_group)
    summed = jnp.einsum('tgn,tge,tgep->gepn', writer, weights, grouped, precision=HIGHEST)
    return summed.reshape(head_count, head_width, state_width)

def group_norm(gated, group_count, group_gain):
    length = gated.shape[0]
    grouped = gated.reshape(length, group_count, -1)
    normed = grouped * lax.rsqrt(lax.optimization_barrier(jnp.mean(grouped * grouped, axis=-1, keepdims=True)) + EPSILON)
    return (normed.reshape(length, -1) * group_gain).astype(jnp.bfloat16)

def reference(latent, context, condition, context_condition, shift_weight, scale_weight, gate_weight, norm_gain, out_gate_weight, signal_weight, writer_weight, reader_matrix, step_weight, signal_taps, writer_taps, reader_taps, step_bias, decay_log, decay_extra, group_gain, output_weight):
    cond_act = jax.nn.silu(jnp.stack([condition, context_condition]).astype(jnp.float32)).astype(jnp.bfloat16)
    shift_vec = jnp.dot(cond_act, shift_weight, preferred_element_type=jnp.float32)
    scale_vec = jnp.dot(cond_act, scale_weight, preferred_element_type=jnp.float32)
    gate_vec = jnp.dot(cond_act[:1], gate_weight, preferred_element_type=jnp.float32)[0]
    hidden = modulate(latent, norm_gain, shift_vec[0], scale_vec[0])
    ctx_hidden = modulate(context, norm_gain, shift_vec[1], scale_vec[1])
    conv_taps = jnp.concatenate([signal_taps, writer_taps, reader_taps], axis=1)
    decay_rates = -jnp.exp(decay_log)[:, None, :]
    ctx_raw, ctx_step_in = project_rows(ctx_hidden, signal_weight, writer_weight, reader_matrix, step_weight)
    ctx_conv = centred_conv(jnp.pad(ctx_raw, ((1, 1), (0, 0))), conv_taps, CTX)
    ctx_signal, ctx_writer, _ = split_mixed(ctx_conv, HEADS, HEAD_DIM, GROUPS, STATE)
    prefix_stride_length = jax.nn.softplus(ctx_step_in.astype(jnp.float32) + step_bias[:, None, :])
    ctx_decay = decay_rates * prefix_stride_length
    cum_log = jnp.cumsum(ctx_decay, axis=1)
    ctx_forward = context_state(ctx_signal, jnp.exp(cum_log[0, -1:] - cum_log[0]) * prefix_stride_length[0], ctx_writer)
    ctx_backward = context_state(ctx_signal, jnp.exp(cum_log[1] - ctx_decay[1]) * prefix_stride_length[1], ctx_writer)
    gate_in = jnp.dot(hidden, out_gate_weight, preferred_element_type=jnp.float32).astype(jnp.bfloat16)
    raw_cols, step_in = project_rows(hidden, signal_weight, writer_weight, reader_matrix, step_weight)
    conv_out = centred_conv(jnp.pad(raw_cols, ((1, 1), (0, 0))), conv_taps, TOKENS)
    signal, writer, reader = split_mixed(conv_out, HEADS, HEAD_DIM, GROUPS, STATE)
    step_size = jax.nn.softplus(step_in.astype(jnp.float32) + step_bias[:, None, :])
    log_decay = decay_rates * step_size + jnp.swapaxes(decay_extra, 1, 2)
    forward_out, _ = state_span(signal, step_size[0], log_decay[0], writer, reader, ctx_forward, BLOCK)
    backward_out, _ = state_span(jnp.flip(signal, 0), jnp.flip(step_size[1], 0), jnp.flip(log_decay[1], 0), jnp.flip(writer, 0), jnp.flip(reader, 0), ctx_backward, BLOCK)
    both = (forward_out + jnp.flip(backward_out, 0)).reshape(TOKENS, -1)
    gated = both * jax.nn.silu(gate_in.astype(jnp.float32))
    normed = group_norm(gated, GROUPS, group_gain)
    mix = jnp.dot(normed, output_weight, preferred_element_type=jnp.float32)
    return (latent.astype(jnp.float32) + gate_vec * mix).astype(jnp.bfloat16)
```

```python
import functools

import jax
import jax.numpy as jnp
from jax import lax
from jax.experimental import pallas as pl
from jax.experimental.pallas import tpu as pltpu
from jax.sharding import PartitionSpec as P

STATE = 128
BLOCK = 128
EPSILON = 1e-06
TILE_N = 256
F32 = jnp.float32
BF16 = jnp.bfloat16
MESH = pl.DeviceIdType.MESH


def silu(v):
    return v / (1.0 + jnp.exp(-v))


def softplus(v):
    return jnp.maximum(v, 0.0) + jnp.log1p(jnp.exp(-jnp.abs(v)))


def dot(a, b):
    return jnp.dot(a, b, preferred_element_type=F32)


def thirds(v):
    first = v.astype(BF16)
    rest = v - first.astype(F32)
    second = rest.astype(BF16)
    third = (rest - second.astype(F32)).astype(BF16)
    return first, second, third


def kernel(dims, *refs):
    (
        latent, context, cond, ctx_cond, shift_w, scale_w, gate_w, gain,
        w_gate, w_sig, w_wr, w_rd, w_step, taps, step_bias, decay_log, extra,
        group_gain, w_out, out,
        lat_v, ctx_v, act, mod_w, mod_part, gate_part, mod_in, gate_in, mod_sum, mod_all,
        scale_rows, shift_rows, edge_out, edge_in, edge_rows, hid, hid_c, w_all, w_st, w_o,
        raw, raw_c, st_raw, cum_col, ecum_col, cum_row, step_row, sig, wr, rd,
        states, dec, ent, ctx_acc, ctx_dec, ctx_send, ctx_recv, cdec_send, cdec_recv,
        span_total, chain_out, chain_in, spread, in_block, normed, acc,
        load_sem, lat_sem, mod_sem, edge_sem, cchain_sem, chain_sem, norm_sem,
    ) = refs
    n, tps, dps = dims
    sp, tp, dp = lax.axis_index("sp"), lax.axis_index("tp"), lax.axis_index("dp")
    place = tp * dps + dp
    places = tps * dps
    width = latent.shape[1]
    half = latent.shape[0]
    length = lat_v.shape[0]
    ctx_len = context.shape[0]
    heads = step_bias.shape[1] // 2
    inner = w_sig.shape[1]
    head_dim = inner // heads
    group_count = w_wr.shape[1] // STATE
    per_group = heads // group_count
    gw = per_group * head_dim
    sw = w_wr.shape[1]
    blocks = length // BLOCK
    mod_rows, mod_cols = shift_w.shape
    out_cols = out.shape[1]

    loads = []

    def load(src, dst):
        c = pltpu.make_async_copy(src, dst, load_sem.at[len(loads)])
        c.start()
        loads.append(c)
        return c

    ld_shift = load(shift_w, mod_w.at[0])
    ld_scale = load(scale_w, mod_w.at[1])
    ld_lat = load(latent, lat_v.at[pl.ds(dp * half, half)])
    ld_ctx = load(context, ctx_v)
    ld_gatew = load(gate_w, mod_w.at[2])
    ld_sig = load(w_sig, w_all.at[:, pl.ds(0, inner)])
    ld_wr = load(w_wr, w_all.at[:, pl.ds(inner, sw)])
    ld_st = load(w_step, w_st)
    ld_rd = load(w_rd, w_all.at[:, pl.ds(inner + sw, sw)])
    ld_gate = load(w_gate, w_all.at[:, pl.ds(inner + 2 * sw, inner)])
    ld_outs = [
        load(w_out.at[pl.ds(q * inner + g * gw, gw)], w_o.at[g, pl.ds(q * gw, gw)])
        for g in range(group_count) for q in range(places)
    ]

    @pl.when(sp == 0)
    def _():
        edge_in[0] = jnp.zeros(edge_in.shape[1:], F32)

    @pl.when(sp == n - 1)
    def _():
        edge_in[1] = jnp.zeros(edge_in.shape[1:], F32)

    barrier = pltpu.get_barrier_semaphore()
    sp_peer = [lax.rem(sp + k, n) for k in range(1, n)]
    tp_peer = [lax.rem(tp + k, tps) for k in range(1, tps)]
    dp_peer = [lax.rem(dp + k, dps) for k in range(1, dps)]
    place_peer = []
    for a in range(tps):
        for b in range(dps):
            if a or b:
                place_peer.append((lax.rem(tp + a, tps), lax.rem(dp + b, dps)))
    for p in sp_peer:
        pl.semaphore_signal(barrier, inc=1, device_id={"sp": p}, device_id_type=MESH)
    for a, b in place_peer:
        pl.semaphore_signal(barrier, inc=1, device_id={"tp": a, "dp": b}, device_id_type=MESH)
    pl.semaphore_wait(barrier, len(sp_peer) + len(place_peer))

    sends = []

    def send(src, dst, ssem, rsem, dev):
        c = pltpu.make_async_remote_copy(
            src_ref=src, dst_ref=dst, send_sem=ssem, recv_sem=rsem,
            device_id=dev, device_id_type=MESH,
        )
        c.start()
        return c

    def arrived(dst, rsem):
        pltpu.make_async_copy(dst, dst, rsem).wait()

    for k, p in enumerate(dp_peer):
        sends.append(send(latent, lat_v.at[pl.ds(dp * half, half)], lat_sem.at[0, k],
                          lat_sem.at[1, dp], {"dp": p}))

    act[...] = jnp.zeros(act.shape, F32)
    act[0:1, :] = silu(cond[...].astype(F32)).astype(BF16).astype(F32)
    act[1:2, :] = silu(ctx_cond[...].astype(F32)).astype(BF16).astype(F32)
    own_act = act[:, pl.ds(pl.multiple_of(sp * mod_rows, 128), mod_rows)].astype(BF16)
    ld_shift.wait()
    mod_part[0:2, :] = dot(own_act, mod_w[0])[0:2]
    ld_scale.wait()
    mod_part[2:4, :] = dot(own_act, mod_w[1])[0:2]
    for k, p in enumerate(sp_peer):
        sends.append(send(mod_part, mod_in.at[sp], mod_sem.at[0, k], mod_sem.at[1, sp], {"sp": p}))
    mod_in[sp] = mod_part[...]
    ld_gatew.wait()
    gate_part[...] = dot(own_act, mod_w[2])[0:1]
    for k, p in enumerate(sp_peer):
        sends.append(send(gate_part, gate_in.at[sp], mod_sem.at[2, k], mod_sem.at[3, sp], {"sp": p}))
    gate_in[sp] = gate_part[...]

    ld_lat.wait()
    ld_ctx.wait()
    for p in dp_peer:
        arrived(lat_v.at[pl.ds(p * half, half)], lat_sem.at[1, p])
    pieces = width // 128
    first_lat = lat_v[0:16, :].astype(F32)[0:1]
    last_lat = lat_v[length - 16:length, :].astype(F32)[15:16]
    first_ctx = ctx_v[0:16, :].astype(F32)[0:1]
    last_ctx = ctx_v[ctx_len - 16:ctx_len, :].astype(F32)[15:16]
    for i in range(pieces):
        cols = slice(i * 128, (i + 1) * 128)
        edge_out[0, 0, i:i + 1, :] = last_lat[:, cols]
        edge_out[0, 1, i:i + 1, :] = last_ctx[:, cols]
        edge_out[1, 0, i:i + 1, :] = first_lat[:, cols]
        edge_out[1, 1, i:i + 1, :] = first_ctx[:, cols]

    def edge_copy(side):
        dev = sp + 1 if side == 0 else sp - 1
        return pltpu.make_async_remote_copy(
            src_ref=edge_out.at[side], dst_ref=edge_in.at[side], send_sem=edge_sem.at[0, side],
            recv_sem=edge_sem.at[1, side], device_id={"sp": dev}, device_id_type=MESH)

    @pl.when(sp < n - 1)
    def _():
        edge_copy(0).start()

    @pl.when(sp > 0)
    def _():
        edge_copy(1).start()

    for p in sp_peer:
        arrived(mod_in.at[p], mod_sem.at[1, p])
    total = mod_in[0]
    for q in range(1, n):
        total = total + mod_in[q]
    mod_sum[...] = total
    for k, (a, b) in enumerate(place_peer):
        sends.append(send(mod_sum, mod_all.at[place], mod_sem.at[4, k], mod_sem.at[5, place],
                          {"tp": a, "dp": b}))
    mod_all[place] = total

    def inv_rms(v):
        return lax.rsqrt(jnp.mean(v * v, axis=-1, keepdims=True) + EPSILON)

    rows_tile = 16

    low_r = lax.broadcasted_iota(jnp.int32, (BLOCK, BLOCK), 0)
    low_c = lax.broadcasted_iota(jnp.int32, (BLOCK, BLOCK), 1)
    lanes2 = 2 * heads
    er = lax.broadcasted_iota(jnp.int32, (lanes2, lanes2 * head_dim), 0)
    ec = lax.broadcasted_iota(jnp.int32, (lanes2, lanes2 * head_dim), 1)
    one = ((ec >= er * head_dim) & (ec < (er + 1) * head_dim)).astype(F32)
    spread[...] = jnp.concatenate([one, one, one], axis=0).astype(BF16)

    def widen(v):
        return jnp.concatenate(thirds(v), axis=1)

    @pl.when(sp > 0)
    def _():
        arrived(edge_in.at[0], edge_sem.at[1, 0])

    @pl.when(sp < n - 1)
    def _():
        arrived(edge_in.at[1], edge_sem.at[1, 1])

    edge_rows[...] = jnp.zeros(edge_rows.shape, F32)
    for i in range(pieces):
        cols = slice(i * 128, (i + 1) * 128)
        edge_rows[0:1, cols] = edge_in[0, 0, i:i + 1, :]
        edge_rows[1:2, cols] = edge_in[1, 0, i:i + 1, :]
        edge_rows[2:3, cols] = edge_in[0, 1, i:i + 1, :]
        edge_rows[3:4, cols] = edge_in[1, 1, i:i + 1, :]

    for a, b in place_peer:
        arrived(mod_all.at[a * dps + b], mod_sem.at[5, a * dps + b])
    for j in range(places):
        cols = slice(j * mod_cols, (j + 1) * mod_cols)
        block_mod = mod_all[j]
        g = gain[0:1, cols]
        for r in range(2):
            shift_rows[r, :, cols] = jnp.broadcast_to(block_mod[r:r + 1], (8, mod_cols))
            scale_rows[r, :, cols] = jnp.broadcast_to((1.0 + block_mod[2 + r:3 + r]) * g, (8, mod_cols))

    def modulated(v, which):
        v3 = v.reshape(-1, 8, width)
        r3 = inv_rms(v).reshape(-1, 8, 1)
        return (v3 * r3 * scale_rows[which][None] + shift_rows[which][None]).reshape(v.shape)

    def ctx_rows(t, carry):
        at = pl.ds(pl.multiple_of(t * rows_tile, rows_tile), rows_tile)
        hid_c[at, :] = modulated(ctx_v[at, :].astype(F32), 1).astype(BF16)
        return carry

    lax.fori_loop(0, ctx_len // rows_tile, ctx_rows, 0)
    edges_lat = modulated(edge_rows[...], 0)
    edges_ctx = modulated(edge_rows[...], 1)
    is_lat = lax.broadcasted_iota(jnp.int32, edges_lat.shape, 0) < 2
    edge_hid = jnp.where(is_lat, edges_lat, edges_ctx)
    hid_c[ctx_len:ctx_len + 16, :] = jnp.concatenate([edge_hid, jnp.zeros_like(edge_hid)], axis=0).astype(BF16)

    ld_sig.wait()
    ld_wr.wait()
    ld_rd.wait()
    conv_tiles = (inner + 2 * sw) // TILE_N
    ridx = lax.broadcasted_iota(jnp.int32, (16, TILE_N), 0)
    has_above = (sp > 0).astype(F32)
    has_below = (sp < n - 1).astype(F32)

    def ctx_proj(t, carry):
        cols = pl.ds(pl.multiple_of(t * TILE_N, TILE_N), TILE_N)
        got = dot(hid_c[...], w_all[:, cols]).astype(BF16).astype(F32)
        raw_c[8:8 + ctx_len, cols] = got[0:ctx_len]
        edges = got[ctx_len:ctx_len + 8]
        raw[0:8, cols] = jnp.broadcast_to(edges[0:1] * has_above, (8, TILE_N))
        raw[8 + length:16 + length, cols] = jnp.broadcast_to(edges[1:2] * has_below, (8, TILE_N))
        raw_c[0:8, cols] = jnp.broadcast_to(edges[2:3] * has_above, (8, TILE_N))
        raw_c[8 + ctx_len:16 + ctx_len, cols] = jnp.broadcast_to(edges[3:4] * has_below, (8, TILE_N))
        return carry

    lax.fori_loop(0, conv_tiles, ctx_proj, 0)
    ld_st.wait()
    ctx_step_in = dot(hid_c[...], w_st[...])[0:ctx_len, 0:lanes2].astype(BF16).astype(F32)

    rates = -jnp.exp(decay_log[...])
    lane = lax.broadcasted_iota(jnp.int32, (1, lanes2), 1)
    forward = lane < heads

    def sums(ld, size):
        r = lax.broadcasted_iota(jnp.int32, (size, size), 0)
        c = lax.broadcasted_iota(jnp.int32, (size, size), 1)
        tri = jnp.concatenate([(r >= c).astype(F32), (r <= c).astype(F32)], axis=0).astype(BF16)
        parts = thirds(ld)
        both = dot(tri, parts[0]) + (dot(tri, parts[1]) + dot(tri, parts[2]))
        return jnp.where(forward, both[:size], both[size:])

    def conv(win, cols, size):
        v = (taps[0:1, cols] * win[7:7 + size] + taps[1:2, cols] * win[8:8 + size]
             + taps[2:3, cols] * win[9:9 + size])
        return silu(v)

    def widened(v, cols):
        return dot(widen(v), spread[:, cols])

    def span_states(sig_g, wr_g, w_f, w_b):
        rhs = jnp.concatenate([sig_g * w_f, sig_g * w_b], axis=1).astype(BF16)
        return lax.dot_general(wr_g, rhs, (((0,), (0,)), ((), ())), preferred_element_type=F32)

    ctx_step = softplus(ctx_step_in + step_bias[...])
    ctx_ld = rates * ctx_step
    ctx_cum = sums(ctx_ld, ctx_len)
    ctx_end = jnp.where(forward, ctx_cum[ctx_len - 1:ctx_len], ctx_cum[0:1])
    ctx_w = jnp.exp(ctx_end - ctx_cum) * ctx_step
    ctx_dec8 = jnp.broadcast_to(jnp.exp(ctx_end), (8, lanes2))
    fwd_all, bwd_all = slice(0, inner), slice(inner, 2 * inner)
    cdf = widened(ctx_dec8, fwd_all)
    cdb = widened(ctx_dec8, bwd_all)
    ctx_states = []
    for g in range(group_count):
        gc = slice(g * gw, (g + 1) * gw)
        bc = slice(inner + g * gw, inner + (g + 1) * gw)
        wc = slice(inner + g * STATE, inner + (g + 1) * STATE)
        sig_g = conv(raw_c[:, gc], gc, ctx_len)
        wr_g = conv(raw_c[:, wc], wc, ctx_len).astype(BF16)
        ctx_states.append(span_states(sig_g, wr_g, widened(ctx_w, gc), widened(ctx_w, bc)))

    def ctx_copy(side):
        dev = sp - 1 if side == 0 else sp + 1
        return [pltpu.make_async_remote_copy(
            src_ref=s.at[side], dst_ref=d.at[side], send_sem=cchain_sem.at[0, side, i],
            recv_sem=cchain_sem.at[1, side, i], device_id={"sp": dev}, device_id_type=MESH)
            for i, (s, d) in enumerate(((ctx_send, ctx_recv), (cdec_send, cdec_recv)))]

    ctx_acc[0] = jnp.concatenate([s[:, :gw] for s in ctx_states], axis=1)
    ctx_acc[1] = jnp.concatenate([s[:, gw:] for s in ctx_states], axis=1)
    ctx_dec[0] = cdf
    ctx_dec[1] = cdb
    ctx_starts = (n - 1, 0)
    for side in range(2):
        @pl.when(sp == ctx_starts[side])
        def _():
            ctx_send[side] = ctx_acc[side].astype(BF16)
            cdec_send[side] = ctx_dec[side]
            if n > 1:
                for c in ctx_copy(side):
                    c.start()

    def lat_rows(t, carry):
        at = pl.ds(pl.multiple_of(t * rows_tile, rows_tile), rows_tile)
        hid[at, :] = modulated(lat_v[at, :].astype(F32), 0).astype(BF16)
        return carry

    lax.fori_loop(0, length // rows_tile, lat_rows, 0)
    ld_gate.wait()

    def lat_proj(t, carry):
        cols = pl.ds(pl.multiple_of(t * TILE_N, TILE_N), TILE_N)
        raw[8:8 + length, cols] = dot(hid[...], w_all[:, cols]).astype(BF16).astype(F32)
        return carry

    state_tiles = (inner + sw) // TILE_N
    all_tiles = (2 * inner + 2 * sw) // TILE_N

    def ctx_hop(hop):
        for side in range(2):
            @pl.when(sp == (n - 1 - hop if side == 0 else hop))
            def _():
                arrived(ctx_recv.at[side], cchain_sem.at[1, side, 0])
                arrived(cdec_recv.at[side], cchain_sem.at[1, side, 1])
                ctx_acc[side] = (ctx_recv[side].astype(F32)
                                 + cdec_recv[side, 0:1] * ctx_acc[side])
                if hop < n - 1:
                    ctx_send[side] = ctx_acc[side].astype(BF16)
                    cdec_send[side] = cdec_recv[side] * ctx_dec[side]
                    for c in ctx_copy(side):
                        c.start()

    st_raw[...] = dot(hid[...], w_st[...]).astype(BF16).astype(F32)
    if n > 1:
        ctx_hop(1)
    lax.fori_loop(0, state_tiles, lat_proj, 0)
    for hop in range(2, n):
        ctx_hop(hop)

    def lat_block(b, carry):
        at = pl.ds(pl.multiple_of(b * BLOCK, BLOCK), BLOCK)
        window = pl.ds(pl.multiple_of(b * BLOCK, BLOCK), BLOCK + 16)
        step = softplus(st_raw[at, 0:lanes2] + step_bias[...])
        ld = rates * step + extra[:, at].T
        cum = sums(ld, BLOCK)
        end = jnp.where(forward, cum[BLOCK - 1:BLOCK], cum[0:1])
        weight = jnp.exp(end - cum) * step
        cum_col[b] = cum
        ecum_col[b] = jnp.exp(cum)
        cum_row[b] = cum.T
        step_row[b] = step.T
        end8 = jnp.broadcast_to(jnp.exp(end), (8, lanes2))
        dec[b] = widened(end8, slice(0, 2 * inner))
        for g in range(group_count):
            gc = slice(g * gw, (g + 1) * gw)
            bc = slice(inner + g * gw, inner + (g + 1) * gw)
            wc = slice(inner + g * STATE, inner + (g + 1) * STATE)
            sig_g = conv(raw[window, gc], gc, BLOCK)
            wr_g = conv(raw[window, wc], wc, BLOCK).astype(BF16)
            sig[at, gc] = sig_g.astype(BF16)
            wr[at, g * STATE:(g + 1) * STATE] = wr_g
            states[b, g] = span_states(sig_g, wr_g, widened(weight, gc), widened(weight, bc))
        return carry

    lax.fori_loop(0, blocks, lat_block, 0)

    def group_cols(side, g):
        return slice(side * inner + g * gw, side * inner + (g + 1) * gw)

    def block_at(side, i):
        return i if side == 0 else blocks - 1 - i

    def side_cols(side):
        return slice(side * gw, (side + 1) * gw)

    for g in range(group_count):
        for side in range(2):
            def total_step(i, run):
                b = block_at(side, i)
                return run * dec[b, 0:1, group_cols(side, g)] + states[b, g, :, side_cols(side)]

            span_total[side, g] = lax.fori_loop(0, blocks, total_step, jnp.zeros((STATE, gw), F32))
    dec_all = dec[0]
    for b in range(1, blocks):
        dec_all = dec_all * dec[b]

    def chain_copy(side, g):
        dev = sp + 1 if side == 0 else sp - 1
        return pltpu.make_async_remote_copy(
            src_ref=chain_out.at[side, g], dst_ref=chain_in.at[side, g],
            send_sem=chain_sem.at[0, side, g], recv_sem=chain_sem.at[1, side, g],
            device_id={"sp": dev}, device_id_type=MESH)

    def chain_hop(hop):
        for side in range(2):
            for g in range(group_count):
                @pl.when(sp == (hop if side == 0 else n - 1 - hop))
                def _():
                    if hop == 0:
                        chain_in[side, g] = ctx_acc[side, :, g * gw:(g + 1) * gw].astype(BF16)
                    else:
                        arrived(chain_in.at[side, g], chain_sem.at[1, side, g])
                    if hop < n - 1:
                        chain_out[side, g] = (
                            chain_in[side, g].astype(F32) * dec_all[0:1, group_cols(side, g)]
                            + span_total[side, g]).astype(BF16)
                        chain_copy(side, g).start()

    def reader_block(b, carry):
        window = pl.ds(pl.multiple_of(b * BLOCK, BLOCK), BLOCK + 16)
        at = pl.ds(pl.multiple_of(b * BLOCK, BLOCK), BLOCK)
        cr, sr, cc = cum_row[b], step_row[b], cum_col[b]
        lane_g = lax.broadcasted_iota(jnp.int32, (BLOCK, gw), 1)
        for g in range(group_count):
            gc = slice(g * gw, (g + 1) * gw)
            rc = slice(inner + sw + g * STATE, inner + sw + (g + 1) * STATE)
            rd_g = conv(raw[window, rc], rc, BLOCK).astype(BF16)
            rd[at, g * STATE:(g + 1) * STATE] = rd_g
            wr_g = wr[at, g * STATE:(g + 1) * STATE]
            sig_g = sig[at, gc]
            pair = lax.dot_general(rd_g, wr_g, (((1,), (1,)), ((), ())), preferred_element_type=F32)
            mixes, sigs = [], []
            for e in range(per_group):
                f, k = g * per_group + e, heads + g * per_group + e
                gap = jnp.where(low_r >= low_c, cc[:, f:f + 1] - cr[f:f + 1], cc[:, k:k + 1] - cr[k:k + 1])
                sf, sk = sr[f:f + 1], sr[k:k + 1]
                size = jnp.where(low_r > low_c, sf, jnp.where(low_r < low_c, sk, sf + sk))
                mixes.append((jnp.exp(gap) * size * pair).astype(BF16))
                mine = (lane_g >= e * head_dim) & (lane_g < (e + 1) * head_dim)
                sigs.append(jnp.where(mine, sig_g, jnp.zeros_like(sig_g)))
            in_block[at, gc] = dot(jnp.concatenate(mixes, axis=1), jnp.concatenate(sigs, axis=0))
        return carry

    chain_hop(0)
    lax.fori_loop(state_tiles, all_tiles - 1, lat_proj, 0)
    if n > 1:
        chain_hop(1)
    lax.fori_loop(all_tiles - 1, all_tiles, lat_proj, 0)
    if n > 2:
        chain_hop(2)
    lax.fori_loop(0, blocks, reader_block, 0)
    for hop in range(3, n):
        chain_hop(hop)

    for p in sp_peer:
        arrived(gate_in.at[p], mod_sem.at[3, p])
    gate_vec = gate_in[0]
    for q in range(1, n):
        gate_vec = gate_vec + gate_in[q]

    chunk = pl.ds(pl.multiple_of(place * gw, 128), gw)

    def norm_copy(g, b, cols, dev, slot, sender):
        ref = normed.at[g, pl.ds(pl.multiple_of(b * BLOCK, BLOCK), BLOCK), cols]
        return pltpu.make_async_remote_copy(
            src_ref=ref, dst_ref=ref, send_sem=norm_sem.at[0, slot, g, b],
            recv_sem=norm_sem.at[1, sender, g, b], device_id=dev, device_id_type=MESH)

    def place_cols(q):
        return pl.ds(pl.multiple_of(q * gw, 128), gw)

    for g in range(group_count):
        gc = slice(g * gw, (g + 1) * gw)
        for side in range(2):
            def enter(i, run):
                b = block_at(side, i)
                ent[b, g, :, side_cols(side)] = run.astype(BF16)
                return run * dec[b, 0:1, group_cols(side, g)] + states[b, g, :, side_cols(side)]

            lax.fori_loop(0, blocks, enter, chain_in[side, g].astype(F32))

        def finish(b, carry):
            at = pl.ds(pl.multiple_of(b * BLOCK, BLOCK), BLOCK)
            at8 = pl.ds(pl.multiple_of(b * BLOCK, BLOCK) + 8, BLOCK)
            carried = dot(rd[at, g * STATE:(g + 1) * STATE], ent[b, g])
            grown = widen(ecum_col[b])
            both = (in_block[at, gc]
                    + carried[:, :gw] * dot(grown, spread[:, group_cols(0, g)])
                    + carried[:, gw:] * dot(grown, spread[:, group_cols(1, g)]))
            start = 1 * inner + 2 * sw + g * gw
            gated = both * silu(raw[at8, start:start + gw])
            done = gated * inv_rms(gated) * group_gain[0:1, gc]
            normed[g, at, chunk] = done.astype(BF16)
            for k, a in enumerate(tp_peer):
                norm_copy(g, b, chunk, {"tp": a}, k, place).start()
            for k, p in enumerate(dp_peer):
                norm_copy(g, b, chunk, {"dp": p}, tps - 1 + k, place).start()
            return carry

        lax.fori_loop(0, blocks, finish, 0)

    for c in ld_outs:
        c.wait()
    own_out = pl.ds(pl.multiple_of(place * out_cols, 128), out_cols)
    slots = (tps - 1) + (dps - 1)
    for g in range(group_count):
        def project(b, carry):
            at = pl.ds(pl.multiple_of(b * BLOCK, BLOCK), BLOCK)
            for k, a in enumerate(tp_peer):
                q = a * dps + dp
                norm_copy(g, b, place_cols(q), {"tp": a}, 0, q).wait_recv()
                for j, p in enumerate(dp_peer):
                    slot = slots + k * (dps - 1) + j
                    norm_copy(g, b, place_cols(q), {"dp": p}, slot, q).start()
            for p in dp_peer:
                for a in range(tps):
                    q = a * dps + p
                    norm_copy(g, b, place_cols(q), {"dp": p}, 0, q).wait_recv()
            part = dot(normed[g, at, :], w_o[g])
            if g > 0:
                part = part + acc[at, :]
            if g < group_count - 1:
                acc[at, :] = part
            else:
                kept = lat_v[at, own_out].astype(F32)
                out[at, :] = (kept + gate_vec * part).astype(BF16)
            return carry

        lax.fori_loop(0, blocks, project, 0)

    for c in sends:
        c.wait_send()

    @pl.when(sp < n - 1)
    def _():
        edge_copy(0).wait_send()

    @pl.when(sp > 0)
    def _():
        edge_copy(1).wait_send()

    for side in range(2):
        @pl.when(sp != ctx_starts[1 - side])
        def _():
            for c in ctx_copy(side):
                c.wait_send()

        @pl.when(sp != ctx_starts[side])
        def _():
            for g in range(group_count):
                chain_copy(side, g).wait_send()

    for g in range(group_count):
        def drained(b, carry):
            for k, a in enumerate(tp_peer):
                norm_copy(g, b, chunk, {"tp": a}, k, place).wait_send()
            for k, p in enumerate(dp_peer):
                norm_copy(g, b, chunk, {"dp": p}, tps - 1 + k, place).wait_send()
            for k, a in enumerate(tp_peer):
                for j, p in enumerate(dp_peer):
                    slot = slots + k * (dps - 1) + j
                    norm_copy(g, b, place_cols(a * dps + dp), {"dp": p}, slot, place).wait_send()
            return carry

        lax.fori_loop(0, blocks, drained, 0)


def on_device(dims, *args):
    (
        latent, context, condition, context_condition, shift_weight, scale_weight, gate_weight,
        norm_gain, out_gate_weight, signal_weight, writer_weight, reader_matrix, step_weight,
        signal_taps, writer_taps, reader_taps, step_bias, decay_log, decay_extra, group_gain,
        output_weight,
    ) = args
    n, tps, dps = dims
    half, width = latent.shape
    length = half * dps
    ctx_len = context.shape[0]
    heads = step_bias.shape[1]
    inner = signal_weight.shape[1]
    sw = writer_weight.shape[1]
    groups = sw // STATE
    gw = inner // groups
    blocks = length // BLOCK
    places = tps * dps
    mod_rows, mod_cols = shift_weight.shape
    out_cols = output_weight.shape[1]
    lanes2 = 2 * heads
    conv_cols = inner + 2 * sw
    steps = jnp.concatenate([step_weight[0], step_weight[1]], axis=1)
    steps = jnp.pad(steps, ((0, 0), (0, 128 - lanes2)))
    taps = jnp.concatenate([signal_taps, writer_taps, reader_taps], axis=1)
    hbm = pl.BlockSpec(memory_space=pl.ANY)
    vmem = pl.BlockSpec(memory_space=pltpu.VMEM)
    slots = (tps - 1) + (dps - 1) + (tps - 1) * (dps - 1)
    peers = max(n - 1, places - 1, 1)
    scratch = [
        pltpu.VMEM((length, width), BF16),
        pltpu.VMEM((ctx_len, width), BF16),
        pltpu.VMEM((8, width), F32),
        pltpu.VMEM((3, mod_rows, mod_cols), BF16),
        pltpu.VMEM((4, mod_cols), F32),
        pltpu.VMEM((1, mod_cols), F32),
        pltpu.VMEM((n, 4, mod_cols), F32),
        pltpu.VMEM((n, 1, mod_cols), F32),
        pltpu.VMEM((4, mod_cols), F32),
        pltpu.VMEM((places, 4, mod_cols), F32),
        pltpu.VMEM((2, 8, width), F32),
        pltpu.VMEM((2, 8, width), F32),
        pltpu.VMEM((2, 2, width // 128, 128), F32),
        pltpu.VMEM((2, 2, width // 128, 128), F32),
        pltpu.VMEM((8, width), F32),
        pltpu.VMEM((length, width), BF16),
        pltpu.VMEM((ctx_len + 16, width), BF16),
        pltpu.VMEM((width, 2 * inner + 2 * sw), BF16),
        pltpu.VMEM((width, 128), BF16),
        pltpu.VMEM((groups, places * gw, out_cols), BF16),
        pltpu.VMEM((length + 16, 2 * inner + 2 * sw), F32),
        pltpu.VMEM((ctx_len + 16, conv_cols), F32),
        pltpu.VMEM((length, 128), F32),
        pltpu.VMEM((blocks, BLOCK, lanes2), F32),
        pltpu.VMEM((blocks, BLOCK, lanes2), F32),
        pltpu.VMEM((blocks, lanes2, BLOCK), F32),
        pltpu.VMEM((blocks, lanes2, BLOCK), F32),
        pltpu.VMEM((length, inner), BF16),
        pltpu.VMEM((length, sw), BF16),
        pltpu.VMEM((length, sw), BF16),
        pltpu.VMEM((blocks, groups, STATE, 2 * gw), F32),
        pltpu.VMEM((blocks, 8, 2 * inner), F32),
        pltpu.VMEM((blocks, groups, STATE, 2 * gw), BF16),
        pltpu.VMEM((2, STATE, inner), F32),
        pltpu.VMEM((2, 8, inner), F32),
        pltpu.VMEM((2, STATE, inner), BF16),
        pltpu.VMEM((2, STATE, inner), BF16),
        pltpu.VMEM((2, 8, inner), F32),
        pltpu.VMEM((2, 8, inner), F32),
        pltpu.VMEM((2, groups, STATE, gw), F32),
        pltpu.VMEM((2, groups, STATE, gw), BF16),
        pltpu.VMEM((2, groups, STATE, gw), BF16),
        pltpu.VMEM((3 * lanes2, 2 * inner), BF16),
        pltpu.VMEM((length, inner), F32),
        pltpu.VMEM((groups, length, places * gw), BF16),
        pltpu.VMEM((length, out_cols), F32),
        pltpu.SemaphoreType.DMA((10 + groups * places,)),
        pltpu.SemaphoreType.DMA((2, dps)),
        pltpu.SemaphoreType.DMA((6, max(n, places))),
        pltpu.SemaphoreType.DMA((2, 2)),
        pltpu.SemaphoreType.DMA((2, 2, 2)),
        pltpu.SemaphoreType.DMA((2, 2, groups)),
        pltpu.SemaphoreType.DMA((2, max(slots, places), groups, blocks)),
    ]
    specs = [hbm, hbm, vmem, vmem, hbm, hbm, hbm, vmem, hbm, hbm, hbm, hbm, hbm,
             vmem, vmem, vmem, vmem, vmem, hbm]
    return pl.pallas_call(
        functools.partial(kernel, dims),
        out_shape=jax.ShapeDtypeStruct((length, out_cols), BF16),
        in_specs=specs,
        out_specs=vmem,
        scratch_shapes=scratch,
        compiler_params=pltpu.CompilerParams(
            collective_id=0, has_side_effects=True, vmem_limit_bytes=67043328),
    )(
        latent, context, condition.reshape(1, -1), context_condition.reshape(1, -1), shift_weight,
        scale_weight, gate_weight, norm_gain.reshape(1, -1), out_gate_weight, signal_weight,
        writer_weight, reader_matrix, steps, taps, step_bias.reshape(1, lanes2),
        decay_log.reshape(1, lanes2), decay_extra.reshape(lanes2, length),
        group_gain.reshape(1, -1), output_weight,
    )


def solution(mesh):
    dims = (mesh.shape["sp"], mesh.shape["tp"], mesh.shape["dp"])
    in_specs = (
        P(("grp", "sp", "dp"), None),
        P(("grp", "sp"), None),
        P("grp"),
        P(),
        P("sp", ("tp", "dp")),
        P("sp", ("tp", "dp")),
        P("sp", ("tp", "dp")),
        P(),
        P(None, ("tp", "dp")),
        P(None, ("tp", "dp")),
        P(None, ("tp", "dp")),
        P(None, ("tp", "dp")),
        P(None, None, ("tp", "dp")),
        P(None, ("tp", "dp")),
        P(None, ("tp", "dp")),
        P(None, ("tp", "dp")),
        P(None, ("tp", "dp")),
        P(None, ("tp", "dp")),
        P(None, ("tp", "dp"), ("grp", "sp")),
        P(("tp", "dp")),
        P(None, ("tp", "dp")),
    )
    out_specs = P(("grp", "sp"), ("tp", "dp"))
    return jax.shard_map(
        functools.partial(on_device, dims), mesh=mesh, in_specs=in_specs, out_specs=out_specs,
        check_vma=False,
    )
```

```python
import functools

import jax
import jax.numpy as jnp
from jax import lax
from jax.experimental import pallas as pl
from jax.experimental.pallas import tpu as pltpu
from jax.sharding import PartitionSpec as P

STATE = 128
BLOCK = 128
EPSILON = 1e-06
TILE_N = 512
F32 = jnp.float32
BF16 = jnp.bfloat16
MESH = pl.DeviceIdType.MESH


def silu(v):
    return v / (1.0 + jnp.exp(-v))


def softplus(v):
    return jnp.maximum(v, 0.0) + jnp.log1p(jnp.exp(-jnp.abs(v)))


def dot(a, b):
    return jnp.dot(a, b, preferred_element_type=F32)


def dot_t(a, b):
    return lax.dot_general(a, b, (((1,), (1,)), ((), ())), preferred_element_type=F32)


def thirds(v):
    first = v.astype(BF16)
    rest = v - first.astype(F32)
    second = rest.astype(BF16)
    third = (rest - second.astype(F32)).astype(BF16)
    return first, second, third


def kernel(dims, *refs):
    (
        latent, context, cond, ctx_cond, shift_w, scale_w, gate_w, gain,
        w_gate, w_sig, w_wr, w_rd, w_step, sig_taps, wr_taps, rd_taps, step_bias, decay_log, extra,
        group_gain, w_out, out,
        lat_v, ctx_v, act, mod_w, mod_part, gate_part, mod_in, gate_in, mod_sum, mod_all,
        scale_rows, shift_rows, edge_out, edge_in, edge_rows, hid, hid_c, w_all, w_st, w_o,
        raw, raw_c, gates, lat_rms, ctx_rms, cum_col, ecum_col, weight_col, cum_row, step_row, sig, wr, rd,
        states, dec, ent, ctx_acc, ctx_dec, ctx_send, ctx_recv, cdec_send, cdec_recv,
        span_total, chain_out, chain_in, spread, in_block, normed, acc,
        load_sem, lat_sem, mod_sem, edge_sem, cchain_sem, chain_sem, norm_sem,
    ) = refs
    n, tps, dps = dims
    sp, tp, dp = lax.axis_index("sp"), lax.axis_index("tp"), lax.axis_index("dp")
    place = tp * dps + dp
    places = tps * dps
    width = latent.shape[1]
    half = latent.shape[0]
    length = lat_v.shape[0]
    ctx_len = context.shape[0]
    heads = step_bias.shape[1]
    inner = w_sig.shape[1]
    head_dim = inner // heads
    group_count = w_wr.shape[1] // STATE
    per_group = heads // group_count
    gw = per_group * head_dim
    sw = w_wr.shape[1]
    blocks = length // BLOCK
    mod_rows, mod_cols = shift_w.shape
    out_cols = out.shape[1]

    loads = []

    def load(src, dst):
        c = pltpu.make_async_copy(src, dst, load_sem.at[len(loads)])
        c.start()
        loads.append(c)
        return c

    ld_shift = load(shift_w, mod_w.at[0])
    ld_scale = load(scale_w, mod_w.at[1])
    ld_lat = load(latent, lat_v.at[pl.ds(dp * half, half)])
    ld_ctx = load(context, ctx_v)
    ld_gatew = load(gate_w, mod_w.at[2])
    ld_sig = load(w_sig, w_all.at[:, pl.ds(sw, inner)])
    ld_wr = load(w_wr, w_all.at[:, pl.ds(0, sw)])
    ld_st = load(w_step, w_st)
    ld_rd = load(w_rd, w_all.at[:, pl.ds(inner + sw, sw)])
    ld_gate = load(w_gate, w_all.at[:, pl.ds(inner + 2 * sw, inner)])
    ld_outs = [
        load(w_out.at[pl.ds(q * inner + g * gw, gw)], w_o.at[g, pl.ds(q * gw, gw)])
        for g in range(group_count) for q in range(places)
    ]

    @pl.when(sp == 0)
    def _():
        edge_in[0] = jnp.zeros(edge_in.shape[1:], F32)

    @pl.when(sp == n - 1)
    def _():
        edge_in[1] = jnp.zeros(edge_in.shape[1:], F32)

    barrier = pltpu.get_barrier_semaphore()
    sp_peer = [lax.rem(sp + k, n) for k in range(1, n)]
    tp_peer = [lax.rem(tp + k, tps) for k in range(1, tps)]
    dp_peer = [lax.rem(dp + k, dps) for k in range(1, dps)]
    place_peer = []
    for a in range(tps):
        for b in range(dps):
            if a or b:
                place_peer.append((lax.rem(tp + a, tps), lax.rem(dp + b, dps)))
    for p in sp_peer:
        pl.semaphore_signal(barrier, inc=1, device_id={"sp": p}, device_id_type=MESH)
    for a, b in place_peer:
        pl.semaphore_signal(barrier, inc=1, device_id={"tp": a, "dp": b}, device_id_type=MESH)
    sends = []

    def send(src, dst, ssem, rsem, dev):
        c = pltpu.make_async_remote_copy(
            src_ref=src, dst_ref=dst, send_sem=ssem, recv_sem=rsem,
            device_id=dev, device_id_type=MESH,
        )
        c.start()
        return c

    def arrived(dst, rsem):
        pltpu.make_async_copy(dst, dst, rsem).wait()

    act[...] = jnp.zeros(act.shape, F32)
    act[0:1, :] = silu(cond[...].astype(F32)).astype(BF16).astype(F32).reshape(1, -1)
    act[1:2, :] = silu(ctx_cond[...].astype(F32)).astype(BF16).astype(F32).reshape(1, -1)
    own_act = act[:, pl.ds(pl.multiple_of(sp * mod_rows, 128), mod_rows)].astype(BF16)
    ld_shift.wait()
    mod_part[0:2, :] = dot(own_act, mod_w[0])[0:2]
    ld_scale.wait()
    mod_part[2:4, :] = dot(own_act, mod_w[1])[0:2]
    pl.semaphore_wait(barrier, len(sp_peer) + len(place_peer))
    for k, p in enumerate(sp_peer):
        sends.append(send(mod_part, mod_in.at[sp], mod_sem.at[0, k], mod_sem.at[1, sp], {"sp": p}))
    mod_in[sp] = mod_part[...]

    for k, p in enumerate(dp_peer):
        sends.append(send(latent, lat_v.at[pl.ds(dp * half, half)], lat_sem.at[0, k],
                          lat_sem.at[1, dp], {"dp": p}))

    def inv_rms(v):
        return lax.rsqrt(jnp.mean(v * v, axis=-1, keepdims=True) + EPSILON)

    def row_tile(rows):
        return min(rows, 64)

    def rms_rows(ref, keep, start, count):
        tile = row_tile(count)

        def step(t, carry):
            at = pl.ds(pl.multiple_of(start + t * tile, tile), tile)
            total = jnp.zeros((tile, 128), F32)
            for c in range(width // 128):
                v = ref[at, c * 128:(c + 1) * 128].astype(F32)
                total = total + v * v
            mean = jnp.sum(total, axis=-1, keepdims=True) * (1.0 / width)
            keep[at, :] = jnp.broadcast_to(lax.rsqrt(mean + EPSILON), (tile, 128))
            return carry

        lax.fori_loop(0, count // tile, step, 0)

    ld_lat.wait()
    rms_rows(lat_v, lat_rms, dp * half, half)

    for p in sp_peer:
        arrived(mod_in.at[p], mod_sem.at[1, p])
    total = mod_in[0]
    for q in range(1, n):
        total = total + mod_in[q]
    mod_sum[...] = total
    for k, (a, b) in enumerate(place_peer):
        sends.append(send(mod_sum, mod_all.at[place], mod_sem.at[4, k], mod_sem.at[5, place],
                          {"tp": a, "dp": b}))
    mod_all[place] = total

    ld_ctx.wait()
    for p in dp_peer:
        arrived(lat_v.at[pl.ds(p * half, half)], lat_sem.at[1, p])
    pieces = width // 128
    first_lat = lat_v[0:16, :].astype(F32)[0:1]
    last_lat = lat_v[length - 16:length, :].astype(F32)[15:16]
    first_ctx = ctx_v[0:16, :].astype(F32)[0:1]
    last_ctx = ctx_v[ctx_len - 16:ctx_len, :].astype(F32)[15:16]
    for i in range(pieces):
        cols = slice(i * 128, (i + 1) * 128)
        edge_out[0, 0, i:i + 1, :] = last_lat[:, cols]
        edge_out[0, 1, i:i + 1, :] = last_ctx[:, cols]
        edge_out[1, 0, i:i + 1, :] = first_lat[:, cols]
        edge_out[1, 1, i:i + 1, :] = first_ctx[:, cols]

    def edge_copy(side):
        dev = sp + 1 if side == 0 else sp - 1
        return pltpu.make_async_remote_copy(
            src_ref=edge_out.at[side], dst_ref=edge_in.at[side], send_sem=edge_sem.at[0, side],
            recv_sem=edge_sem.at[1, side], device_id={"sp": dev}, device_id_type=MESH)

    @pl.when(sp < n - 1)
    def _():
        edge_copy(0).start()

    @pl.when(sp > 0)
    def _():
        edge_copy(1).start()

    for p in dp_peer:
        rms_rows(lat_v, lat_rms, p * half, half)
    rms_rows(ctx_v, ctx_rms, 0, ctx_len)
    ld_gatew.wait()
    gate_part[...] = dot(own_act, mod_w[2])[0:1]
    for k, p in enumerate(sp_peer):
        sends.append(send(gate_part, gate_in.at[sp], mod_sem.at[2, k], mod_sem.at[3, sp], {"sp": p}))
    gate_in[sp] = gate_part[...]

    low_r = lax.broadcasted_iota(jnp.int32, (BLOCK, BLOCK), 0)
    low_c = lax.broadcasted_iota(jnp.int32, (BLOCK, BLOCK), 1)
    lanes2 = 2 * heads
    er = lax.broadcasted_iota(jnp.int32, (lanes2, lanes2 * head_dim), 0)
    ec = lax.broadcasted_iota(jnp.int32, (lanes2, lanes2 * head_dim), 1)
    one = ((ec >= er * head_dim) & (ec < (er + 1) * head_dim)).astype(F32)
    spread[...] = jnp.concatenate([one, one, one], axis=0).astype(BF16)

    def widen(v):
        return jnp.concatenate(thirds(v), axis=1)

    for a, b in place_peer:
        arrived(mod_all.at[a * dps + b], mod_sem.at[5, a * dps + b])
    for j in range(places):
        cols = slice(j * mod_cols, (j + 1) * mod_cols)
        block_mod = mod_all[j]
        g = gain[0:1, cols]
        for r in range(2):
            shift_rows[r, :, cols] = jnp.broadcast_to(block_mod[r:r + 1], (8, mod_cols))
            scale_rows[r, :, cols] = jnp.broadcast_to((1.0 + block_mod[2 + r:3 + r]) * g, (8, mod_cols))

    def hidden_rows(ref, keep, goal, which, start, count):
        tile = row_tile(count)

        def step(t, carry):
            at = pl.ds(pl.multiple_of(start + t * tile, tile), tile)
            r3 = keep[at, :].reshape(tile // 8, 8, 128)
            for c in range(width // 128):
                cols = slice(c * 128, (c + 1) * 128)
                v = ref[at, cols].astype(F32).reshape(tile // 8, 8, 128)
                h = v * r3 * scale_rows[which, :, cols][None] + shift_rows[which, :, cols][None]
                goal[at, cols] = h.reshape(tile, 128).astype(BF16)
            return carry

        lax.fori_loop(0, count // tile, step, 0)

    hidden_rows(ctx_v, ctx_rms, hid_c, 1, 0, ctx_len)

    @pl.when(sp > 0)
    def _():
        arrived(edge_in.at[0], edge_sem.at[1, 0])

    @pl.when(sp < n - 1)
    def _():
        arrived(edge_in.at[1], edge_sem.at[1, 1])

    edge_rows[...] = jnp.zeros(edge_rows.shape, F32)
    for i in range(pieces):
        cols = slice(i * 128, (i + 1) * 128)
        edge_rows[0:1, cols] = edge_in[0, 0, i:i + 1, :]
        edge_rows[1:2, cols] = edge_in[1, 0, i:i + 1, :]
        edge_rows[2:3, cols] = edge_in[0, 1, i:i + 1, :]
        edge_rows[3:4, cols] = edge_in[1, 1, i:i + 1, :]
    edge_v = edge_rows[...]
    edge_n = edge_v * inv_rms(edge_v)
    is_lat = lax.broadcasted_iota(jnp.int32, edge_v.shape, 0) < 2
    edge_hid = jnp.where(is_lat, edge_n * scale_rows[0] + shift_rows[0],
                         edge_n * scale_rows[1] + shift_rows[1])
    hid_c[ctx_len:ctx_len + 16, :] = jnp.concatenate([edge_hid, jnp.zeros_like(edge_hid)], axis=0).astype(BF16)

    ld_sig.wait()
    ld_wr.wait()
    ld_rd.wait()
    has_above = (sp > 0).astype(F32)
    has_below = (sp < n - 1).astype(F32)

    def ctx_proj(t, carry):
        cols = pl.ds(pl.multiple_of(t * TILE_N, TILE_N), TILE_N)
        got = dot(hid_c[...], w_all[:, cols]).astype(BF16).astype(F32)
        for i in range(TILE_N // 128):
            c, piece = t * (TILE_N // 128) + i, got[:, i * 128:(i + 1) * 128]
            raw_c[c, 8:8 + ctx_len, :] = piece[0:ctx_len]
            edges = piece[ctx_len:ctx_len + 8]
            raw[c, 0:8, :] = jnp.broadcast_to(edges[0:1] * has_above, (8, 128))
            raw[c, 8 + length:16 + length, :] = jnp.broadcast_to(edges[1:2] * has_below, (8, 128))
            raw_c[c, 0:8, :] = jnp.broadcast_to(edges[2:3] * has_above, (8, 128))
            raw_c[c, 8 + ctx_len:16 + ctx_len, :] = jnp.broadcast_to(edges[3:4] * has_below, (8, 128))
        return carry

    lax.fori_loop(0, (inner + 2 * sw) // TILE_N, ctx_proj, 0)
    ld_st.wait()
    ctx_step_in = dot_t(hid_c[0:ctx_len], w_st[...]).astype(BF16).astype(F32)

    bias = jnp.concatenate([step_bias[0:1], step_bias[1:2]], axis=1)
    rates = -jnp.exp(jnp.concatenate([decay_log[0:1], decay_log[1:2]], axis=1))

    def sums(ld, size):
        r = lax.broadcasted_iota(jnp.int32, (size, size), 0)
        c = lax.broadcasted_iota(jnp.int32, (size, size), 1)
        tri = jnp.concatenate([(r >= c).astype(F32), (r <= c).astype(F32)], axis=0).astype(BF16)
        parts = thirds(ld)
        both = dot(tri, parts[0]) + (dot(tri, parts[1]) + dot(tri, parts[2]))
        lane = lax.broadcasted_iota(jnp.int32, (1, ld.shape[1]), 1)
        forward = lax.rem(lane, lanes2) < heads
        cum = jnp.where(forward, both[:size], both[size:])
        return cum, jnp.where(forward, cum[size - 1:size], cum[0:1])

    def conv(ref, taps, first, start, count, cols, size):
        outs = []
        for i in range(count):
            tc = slice(cols + i * 128, cols + (i + 1) * 128)
            v = (taps[0:1, tc] * ref[first + i, pl.ds(start + 7, size), :]
                 + taps[1:2, tc] * ref[first + i, pl.ds(start + 8, size), :]
                 + taps[2:3, tc] * ref[first + i, pl.ds(start + 9, size), :])
            outs.append(silu(v))
        return outs[0] if count == 1 else jnp.concatenate(outs, axis=1)

    gp, sig_first, rd_first = gw // 128, sw // 128, (inner + sw) // 128

    def widened(v, cols):
        return dot(widen(v), spread[:, cols])

    def span_states(sig_g, wr_g, w_f, w_b):
        rhs = jnp.concatenate([sig_g * w_f, sig_g * w_b], axis=1).astype(BF16)
        return lax.dot_general(wr_g, rhs, (((0,), (0,)), ((), ())), preferred_element_type=F32)

    def group_cols(side, g):
        return slice(side * inner + g * gw, side * inner + (g + 1) * gw)

    ctx_step = softplus(ctx_step_in + bias)
    ctx_cum, ctx_end = sums(rates * ctx_step, ctx_len)
    ctx_w = widen(jnp.exp(ctx_end - ctx_cum) * ctx_step)
    ctx_dec8 = widened(jnp.broadcast_to(jnp.exp(ctx_end), (8, lanes2)), slice(0, 2 * inner))
    ctx_dec[0] = ctx_dec8[:, :inner]
    ctx_dec[1] = ctx_dec8[:, inner:]
    for g in range(group_count):
        sig_g = conv(raw_c, sig_taps, sig_first + g * gp, 0, gp, g * gw, ctx_len)
        wr_g = conv(raw_c, wr_taps, g, 0, 1, g * STATE, ctx_len).astype(BF16)
        got = span_states(sig_g, wr_g, dot(ctx_w, spread[:, group_cols(0, g)]),
                          dot(ctx_w, spread[:, group_cols(1, g)]))
        ctx_acc[0, g] = got[:, :gw]
        ctx_acc[1, g] = got[:, gw:]

    def ctx_copy(side, g):
        dev = sp - 1 if side == 0 else sp + 1
        pairs = [(ctx_send.at[side, g], ctx_recv.at[side, g])]
        if g == 0:
            pairs.append((cdec_send.at[side], cdec_recv.at[side]))
        return [pltpu.make_async_remote_copy(
            src_ref=s, dst_ref=d, send_sem=cchain_sem.at[0, side, g, i],
            recv_sem=cchain_sem.at[1, side, g, i], device_id={"sp": dev}, device_id_type=MESH)
            for i, (s, d) in enumerate(pairs)]

    ctx_starts = (n - 1, 0)
    for side in range(2):
        @pl.when(sp == ctx_starts[side])
        def _():
            cdec_send[side] = ctx_dec[side]
            for g in range(group_count):
                ctx_send[side, g] = ctx_acc[side, g].astype(BF16)
                if n > 1:
                    for c in ctx_copy(side, g):
                        c.start()

    def ctx_hop(hop, g):
        if hop >= n or g >= group_count:
            return
        for side in range(2):
            @pl.when(sp == (n - 1 - hop if side == 0 else hop))
            def _():
                arrived(ctx_recv.at[side, g], cchain_sem.at[1, side, g, 0])
                if g == 0:
                    arrived(cdec_recv.at[side], cchain_sem.at[1, side, 0, 1])
                    if hop < n - 1:
                        cdec_send[side] = cdec_recv[side] * ctx_dec[side]
                ctx_acc[side, g] = (ctx_recv[side, g].astype(F32)
                                    + cdec_recv[side, 0:1, g * gw:(g + 1) * gw] * ctx_acc[side, g])
                if hop < n - 1:
                    ctx_send[side, g] = ctx_acc[side, g].astype(BF16)
                    for c in ctx_copy(side, g):
                        c.start()

    hidden_rows(lat_v, lat_rms, hid, 0, 0, length)
    ctx_hop(1, 0)
    st_raw = dot_t(hid[...], w_st[...]).astype(BF16).astype(F32)

    for g in range(1, group_count):
        ctx_hop(1, g)

    def by_block(v):
        return jnp.concatenate([v] * blocks, axis=1)

    step = softplus(jnp.concatenate([st_raw[b * BLOCK:(b + 1) * BLOCK] for b in range(blocks)], axis=1)
                    + by_block(bias))
    more = jnp.concatenate([extra[:, b * BLOCK:(b + 1) * BLOCK] for b in range(blocks)], axis=0).T
    cum, end = sums(by_block(rates) * step + more, BLOCK)
    weight, grow = jnp.exp(end - cum) * step, jnp.exp(cum)
    cum_t, step_t = cum.T, step.T
    ends = jnp.exp(end)
    for b in range(blocks):
        at_b = slice(b * lanes2, (b + 1) * lanes2)
        cum_col[b] = cum[:, at_b]
        ecum_col[b] = widen(grow[:, at_b])
        weight_col[b] = widen(weight[:, at_b])
        cum_row[b] = cum_t[at_b]
        step_row[b] = step_t[at_b]
        dec[b] = widened(jnp.broadcast_to(ends[:, at_b], (8, lanes2)), slice(0, 2 * inner))
    dec_all = dec[0]
    for b in range(1, blocks):
        dec_all = dec_all * dec[b]

    def project(first, size):
        got = dot(hid[...], w_all[:, first:first + size]).astype(BF16).astype(F32)
        for i in range(size // 128):
            raw[first // 128 + i, 8:8 + length, :] = got[:, i * 128:(i + 1) * 128]

    def gate_project():
        gates[...] = dot(hid[...], w_all[:, inner + 2 * sw:2 * inner + 2 * sw]).astype(BF16)

    def block_at(side, i):
        return i if side == 0 else blocks - 1 - i

    def side_cols(side):
        return slice(side * gw, (side + 1) * gw)

    def group_states(g):
        gc = slice(g * gw, (g + 1) * gw)

        def step(b, carry):
            start = pl.multiple_of(b * BLOCK, BLOCK)
            at = pl.ds(start, BLOCK)
            sig_g = conv(raw, sig_taps, sig_first + g * gp, start, gp, g * gw, BLOCK)
            wr_g = conv(raw, wr_taps, g, start, 1, g * STATE, BLOCK).astype(BF16)
            sig[at, gc] = sig_g.astype(BF16)
            wr[at, g * STATE:(g + 1) * STATE] = wr_g
            wide = weight_col[b]
            states[b, g] = span_states(sig_g, wr_g, dot(wide, spread[:, group_cols(0, g)]),
                                       dot(wide, spread[:, group_cols(1, g)]))
            return carry

        lax.fori_loop(0, blocks, step, 0, unroll=2)
        for side in range(2):
            def total_step(i, run):
                b = block_at(side, i)
                return run * dec[b, 0:1, group_cols(side, g)] + states[b, g, :, side_cols(side)]

            span_total[side, g] = lax.fori_loop(0, blocks, total_step, jnp.zeros((STATE, gw), F32))

    def chain_copy(side, g):
        dev = sp + 1 if side == 0 else sp - 1
        return pltpu.make_async_remote_copy(
            src_ref=chain_out.at[side, g], dst_ref=chain_in.at[side, g],
            send_sem=chain_sem.at[0, side, g], recv_sem=chain_sem.at[1, side, g],
            device_id={"sp": dev}, device_id_type=MESH)

    def chain_hop(hop, g):
        if hop < 0 or hop >= n:
            return
        for side in range(2):
            @pl.when(sp == (hop if side == 0 else n - 1 - hop))
            def _():
                if hop == 0:
                    chain_in[side, g] = ctx_acc[side, g].astype(BF16)
                else:
                    arrived(chain_in.at[side, g], chain_sem.at[1, side, g])
                if hop < n - 1:
                    chain_out[side, g] = (
                        chain_in[side, g].astype(F32) * dec_all[0:1, group_cols(side, g)]
                        + span_total[side, g]).astype(BF16)
                    chain_copy(side, g).start()

    def group_blocks(g):
        gc = slice(g * gw, (g + 1) * gw)

        def step(b, carry):
            start = pl.multiple_of(b * BLOCK, BLOCK)
            at = pl.ds(start, BLOCK)
            cr, sr, cc = cum_row[b], step_row[b], cum_col[b]
            lane_g = lax.broadcasted_iota(jnp.int32, (BLOCK, gw), 1)
            rd_g = conv(raw, rd_taps, rd_first + g, start, 1, g * STATE, BLOCK).astype(BF16)
            rd[at, g * STATE:(g + 1) * STATE] = rd_g
            wr_g = wr[at, g * STATE:(g + 1) * STATE]
            sig_g = sig[at, gc]
            pair = dot_t(rd_g, wr_g)
            mixes, sigs = [], []
            for e in range(per_group):
                f, k = g * per_group + e, heads + g * per_group + e
                gap = jnp.where(low_r >= low_c, cc[:, f:f + 1] - cr[f:f + 1], cc[:, k:k + 1] - cr[k:k + 1])
                sf, sk = sr[f:f + 1], sr[k:k + 1]
                size = jnp.where(low_r > low_c, sf, jnp.where(low_r < low_c, sk, sf + sk))
                mixes.append((jnp.exp(gap) * size * pair).astype(BF16))
                mine = (lane_g >= e * head_dim) & (lane_g < (e + 1) * head_dim)
                sigs.append(jnp.where(mine, sig_g, jnp.zeros_like(sig_g)))
            in_block[at, gc] = dot(jnp.concatenate(mixes, axis=1), jnp.concatenate(sigs, axis=0))
            return carry

        lax.fori_loop(0, blocks, step, 0, unroll=2)

    chunk = pl.ds(pl.multiple_of(place * gw, 128), gw)

    def norm_copy(g, b, cols, dev, slot, sender):
        ref = normed.at[g, pl.ds(pl.multiple_of(b * BLOCK, BLOCK), BLOCK), cols]
        return pltpu.make_async_remote_copy(
            src_ref=ref, dst_ref=ref, send_sem=norm_sem.at[0, slot, g, b],
            recv_sem=norm_sem.at[1, sender, g, b], device_id=dev, device_id_type=MESH)

    def place_cols(q):
        return pl.ds(pl.multiple_of(q * gw, 128), gw)

    def finish_group(g):
        gc = slice(g * gw, (g + 1) * gw)
        for side in range(2):
            def enter(i, run):
                b = block_at(side, i)
                ent[b, g, :, side_cols(side)] = run.astype(BF16)
                return run * dec[b, 0:1, group_cols(side, g)] + states[b, g, :, side_cols(side)]

            lax.fori_loop(0, blocks, enter, chain_in[side, g].astype(F32))

        def finish(b, carry):
            at = pl.ds(pl.multiple_of(b * BLOCK, BLOCK), BLOCK)
            carried = dot(rd[at, g * STATE:(g + 1) * STATE], ent[b, g])
            grown = ecum_col[b]
            both = (in_block[at, gc]
                    + carried[:, :gw] * dot(grown, spread[:, group_cols(0, g)])
                    + carried[:, gw:] * dot(grown, spread[:, group_cols(1, g)]))
            gated = both * silu(gates[at, gc].astype(F32))
            done = gated * inv_rms(gated) * group_gain[0:1, gc]
            normed[g, at, chunk] = done.astype(BF16)
            for k, a in enumerate(tp_peer):
                norm_copy(g, b, chunk, {"tp": a}, k, place).start()
            for k, p in enumerate(dp_peer):
                norm_copy(g, b, chunk, {"dp": p}, tps - 1 + k, place).start()
            return carry

        lax.fori_loop(0, blocks, finish, 0)

    ctx_hop(2, 0)
    project(0, sw + gw)
    for g in range(1, group_count):
        ctx_hop(2, g)
    group_states(0)
    for hop in range(3, n):
        ctx_hop(hop, 0)
    chain_hop(0, 0)
    project(sw + gw, inner + sw - gw)
    chain_hop(1, 0)
    for g in range(1, group_count):
        group_states(g)
        for hop in range(3, n):
            ctx_hop(hop, g)
        chain_hop(0, g)
    ld_gate.wait()
    group_blocks(0)
    chain_hop(2, 0)
    gate_project()
    for g in range(1, group_count):
        chain_hop(1, g)
    for g in range(group_count):
        if g > 0:
            group_blocks(g)
            chain_hop(2, g)
        for hop in range(3, n):
            chain_hop(hop, g)
        finish_group(g)

    for p in sp_peer:
        arrived(gate_in.at[p], mod_sem.at[3, p])
    gate_vec = gate_in[0]
    for q in range(1, n):
        gate_vec = gate_vec + gate_in[q]

    for c in ld_outs:
        c.wait()
    own_out = pl.ds(pl.multiple_of(place * out_cols, 128), out_cols)
    slots = (tps - 1) + (dps - 1)

    def relay(g, b):
        for k, a in enumerate(tp_peer):
            q = a * dps + dp
            norm_copy(g, b, place_cols(q), {"tp": a}, 0, q).wait_recv()
            for j, p in enumerate(dp_peer):
                slot = slots + k * (dps - 1) + j
                norm_copy(g, b, place_cols(q), {"dp": p}, slot, q).start()

    def gathered(g, b):
        for p in dp_peer:
            for a in range(tps):
                q = a * dps + p
                norm_copy(g, b, place_cols(q), {"dp": p}, 0, q).wait_recv()

    for g in range(group_count - 1):
        lax.fori_loop(0, blocks, lambda b, carry: (relay(g, b), carry)[1], 0)
        lax.fori_loop(0, blocks, lambda b, carry: (gathered(g, b), carry)[1], 0)
        part = dot(normed[g], w_o[g])
        acc[...] = part if g == 0 else acc[...] + part

    def finished(first, count):
        g = group_count - 1
        for b in range(first, first + count):
            gathered(g, b)
        at = pl.ds(first * BLOCK, count * BLOCK)
        part = dot(normed[g, at, :], w_o[g])
        if g > 0:
            part = part + acc[at, :]
        kept = lat_v[at, own_out].astype(F32)
        out[at, :] = (kept + gate_vec * part).astype(BF16)

    spans, first = [], 0
    while first < blocks:
        count = 2 if blocks - first > 2 else 1
        spans.append((first, count))
        first += count
    for i, (first, count) in enumerate(spans):
        for b in range(first, first + count):
            relay(group_count - 1, b)
        if i > 0:
            finished(*spans[i - 1])
    finished(*spans[-1])

    for c in sends:
        c.wait_send()

    @pl.when(sp < n - 1)
    def _():
        edge_copy(0).wait_send()

    @pl.when(sp > 0)
    def _():
        edge_copy(1).wait_send()

    for side in range(2):
        @pl.when(sp != ctx_starts[1 - side])
        def _():
            for g in range(group_count):
                for c in ctx_copy(side, g):
                    c.wait_send()

        @pl.when(sp != ctx_starts[side])
        def _():
            for g in range(group_count):
                chain_copy(side, g).wait_send()

    for g in range(group_count):
        def drained(b, carry):
            for k, a in enumerate(tp_peer):
                norm_copy(g, b, chunk, {"tp": a}, k, place).wait_send()
            for k, p in enumerate(dp_peer):
                norm_copy(g, b, chunk, {"dp": p}, tps - 1 + k, place).wait_send()
            for k, a in enumerate(tp_peer):
                for j, p in enumerate(dp_peer):
                    slot = slots + k * (dps - 1) + j
                    norm_copy(g, b, place_cols(a * dps + dp), {"dp": p}, slot, place).wait_send()
            return carry

        lax.fori_loop(0, blocks, drained, 0)


def on_device(dims, *args):
    (
        latent, context, condition, context_condition, shift_weight, scale_weight, gate_weight,
        norm_gain, out_gate_weight, signal_weight, writer_weight, reader_matrix, step_weight,
        signal_taps, writer_taps, reader_taps, step_bias, decay_log, decay_extra, group_gain,
        output_weight,
    ) = args
    n, tps, dps = dims
    half, width = latent.shape
    length = half * dps
    ctx_len = context.shape[0]
    heads = step_bias.shape[1]
    inner = signal_weight.shape[1]
    sw = writer_weight.shape[1]
    groups = sw // STATE
    gw = inner // groups
    blocks = length // BLOCK
    places = tps * dps
    mod_rows, mod_cols = shift_weight.shape
    out_cols = output_weight.shape[1]
    lanes2 = 2 * heads
    conv_cols = inner + 2 * sw
    steps = jnp.swapaxes(step_weight, 1, 2).reshape(lanes2, width)
    hbm = pl.BlockSpec(memory_space=pl.ANY)
    vmem = pl.BlockSpec(memory_space=pltpu.VMEM)
    slots = (tps - 1) + (dps - 1) + (tps - 1) * (dps - 1)
    peers = max(n - 1, places - 1, 1)
    scratch = [
        pltpu.VMEM((length, width), BF16),
        pltpu.VMEM((ctx_len, width), BF16),
        pltpu.VMEM((8, width), F32),
        pltpu.VMEM((3, mod_rows, mod_cols), BF16),
        pltpu.VMEM((4, mod_cols), F32),
        pltpu.VMEM((1, mod_cols), F32),
        pltpu.VMEM((n, 4, mod_cols), F32),
        pltpu.VMEM((n, 1, mod_cols), F32),
        pltpu.VMEM((4, mod_cols), F32),
        pltpu.VMEM((places, 4, mod_cols), F32),
        pltpu.VMEM((2, 8, width), F32),
        pltpu.VMEM((2, 8, width), F32),
        pltpu.VMEM((2, 2, width // 128, 128), F32),
        pltpu.VMEM((2, 2, width // 128, 128), F32),
        pltpu.VMEM((8, width), F32),
        pltpu.VMEM((length, width), BF16),
        pltpu.VMEM((ctx_len + 16, width), BF16),
        pltpu.VMEM((width, 2 * inner + 2 * sw), BF16),
        pltpu.VMEM((lanes2, width), BF16),
        pltpu.VMEM((groups, places * gw, out_cols), BF16),
        pltpu.VMEM((conv_cols // 128, length + 16, 128), F32),
        pltpu.VMEM((conv_cols // 128, ctx_len + 16, 128), F32),
        pltpu.VMEM((length, inner), BF16),
        pltpu.VMEM((length, 128), F32),
        pltpu.VMEM((ctx_len, 128), F32),
        pltpu.VMEM((blocks, BLOCK, lanes2), F32),
        pltpu.VMEM((blocks, BLOCK, 3 * lanes2), BF16),
        pltpu.VMEM((blocks, BLOCK, 3 * lanes2), BF16),
        pltpu.VMEM((blocks, lanes2, BLOCK), F32),
        pltpu.VMEM((blocks, lanes2, BLOCK), F32),
        pltpu.VMEM((length, inner), BF16),
        pltpu.VMEM((length, sw), BF16),
        pltpu.VMEM((length, sw), BF16),
        pltpu.VMEM((blocks, groups, STATE, 2 * gw), F32),
        pltpu.VMEM((blocks, 8, 2 * inner), F32),
        pltpu.VMEM((blocks, groups, STATE, 2 * gw), BF16),
        pltpu.VMEM((2, groups, STATE, gw), F32),
        pltpu.VMEM((2, 8, inner), F32),
        pltpu.VMEM((2, groups, STATE, gw), BF16),
        pltpu.VMEM((2, groups, STATE, gw), BF16),
        pltpu.VMEM((2, 8, inner), F32),
        pltpu.VMEM((2, 8, inner), F32),
        pltpu.VMEM((2, groups, STATE, gw), F32),
        pltpu.VMEM((2, groups, STATE, gw), BF16),
        pltpu.VMEM((2, groups, STATE, gw), BF16),
        pltpu.VMEM((3 * lanes2, 2 * inner), BF16),
        pltpu.VMEM((length, inner), F32),
        pltpu.VMEM((groups, length, places * gw), BF16),
        pltpu.VMEM((length, out_cols), F32),
        pltpu.SemaphoreType.DMA((10 + groups * places,)),
        pltpu.SemaphoreType.DMA((2, dps)),
        pltpu.SemaphoreType.DMA((6, max(n, places))),
        pltpu.SemaphoreType.DMA((2, 2)),
        pltpu.SemaphoreType.DMA((2, 2, groups, 2)),
        pltpu.SemaphoreType.DMA((2, 2, groups)),
        pltpu.SemaphoreType.DMA((2, max(slots, places), groups, blocks)),
    ]
    specs = [hbm, hbm, vmem, vmem, hbm, hbm, hbm, vmem, hbm, hbm, hbm, hbm, hbm,
             vmem, vmem, vmem, vmem, vmem, vmem, vmem, hbm]
    return pl.pallas_call(
        functools.partial(kernel, dims),
        out_shape=jax.ShapeDtypeStruct((length, out_cols), BF16),
        in_specs=specs,
        out_specs=vmem,
        scratch_shapes=scratch,
        compiler_params=pltpu.CompilerParams(
            collective_id=0, has_side_effects=True, vmem_limit_bytes=67043328),
    )(
        latent, context, condition, context_condition, shift_weight,
        scale_weight, gate_weight, norm_gain.reshape(1, -1), out_gate_weight, signal_weight,
        writer_weight, reader_matrix, steps, signal_taps, writer_taps, reader_taps, step_bias,
        decay_log, decay_extra.reshape(lanes2, length),
        group_gain.reshape(1, -1), output_weight,
    )


def solution(mesh):
    dims = (mesh.shape["sp"], mesh.shape["tp"], mesh.shape["dp"])
    in_specs = (
        P(("grp", "sp", "dp"), None),
        P(("grp", "sp"), None),
        P("grp"),
        P(),
        P("sp", ("tp", "dp")),
        P("sp", ("tp", "dp")),
        P("sp", ("tp", "dp")),
        P(),
        P(None, ("tp", "dp")),
        P(None, ("tp", "dp")),
        P(None, ("tp", "dp")),
        P(None, ("tp", "dp")),
        P(None, None, ("tp", "dp")),
        P(None, ("tp", "dp")),
        P(None, ("tp", "dp")),
        P(None, ("tp", "dp")),
        P(None, ("tp", "dp")),
        P(None, ("tp", "dp")),
        P(None, ("tp", "dp"), ("grp", "sp")),
        P(("tp", "dp")),
        P(None, ("tp", "dp")),
    )
    out_specs = P(("grp", "sp"), ("tp", "dp"))
    return jax.shard_map(
        functools.partial(on_device, dims), mesh=mesh, in_specs=in_specs, out_specs=out_specs,
        check_vma=False,
    )
```

```python
import functools

import jax
import jax.numpy as jnp
from jax import lax
from jax.experimental import pallas as pl
from jax.experimental.pallas import tpu as pltpu
from jax.sharding import PartitionSpec as P

STATE = 128
BLOCK = 128
EPSILON = 1e-06
TILE_N = 512
F32 = jnp.float32
BF16 = jnp.bfloat16
MESH = pl.DeviceIdType.MESH


def silu(v):
    return v / (1.0 + jnp.exp(-v))


def softplus(v):
    return jnp.maximum(v, 0.0) + jnp.log1p(jnp.exp(-jnp.abs(v)))


def dot(a, b):
    return jnp.dot(a, b, preferred_element_type=F32)


def dot_t(a, b):
    return lax.dot_general(a, b, (((1,), (1,)), ((), ())), preferred_element_type=F32)


def thirds(v):
    first = v.astype(BF16)
    rest = v - first.astype(F32)
    second = rest.astype(BF16)
    third = (rest - second.astype(F32)).astype(BF16)
    return first, second, third


def kernel(dims, *refs):
    (
        latent, context, cond, ctx_cond, shift_w, scale_w, gate_w, gain,
        w_gate, w_sig, w_wr, w_rd, w_step, sig_taps, wr_taps, rd_taps, step_bias, decay_log, extra,
        group_gain, w_out, out,
        lat_v, ctx_v, act, mod_w, mod_part, gate_part, mod_in, gate_in, mod_sum, mod_all,
        scale_rows, shift_rows, edge_out, edge_in, edge_rows, hid_c, w_all, w_st, w_o,
        raw, raw_c, gates, cum_col, ecum_col, weight_col, cum_row, step_row, sig, wr, rd,
        states, dec, ent, ctx_acc, ctx_send, ctx_recv, cdec_send, cdec_recv, sdec_send, sdec_recv,
        span_total, chain_out, chain_recv, chain_in, spread, in_block, normed,
        load_sem, lat_sem, mod_sem, edge_sem, cchain_sem, chain_sem, norm_sem,
    ) = refs
    n, tps, dps = dims
    sp, tp, dp = lax.axis_index("sp"), lax.axis_index("tp"), lax.axis_index("dp")
    place = tp * dps + dp
    places = tps * dps
    width = latent.shape[1]
    half = latent.shape[0]
    length = lat_v.shape[0]
    ctx_len = context.shape[0]
    heads = step_bias.shape[1]
    inner = w_sig.shape[1]
    head_dim = inner // heads
    group_count = w_wr.shape[1] // STATE
    per_group = heads // group_count
    gw = per_group * head_dim
    sw = w_wr.shape[1]
    blocks = length // BLOCK
    mod_rows, mod_cols = shift_w.shape
    out_cols = out.shape[1]

    loads = []

    def load(src, dst):
        c = pltpu.make_async_copy(src, dst, load_sem.at[len(loads)])
        c.start()
        loads.append(c)
        return c

    ld_shift = load(shift_w, mod_w.at[0])
    ld_scale = load(scale_w, mod_w.at[1])

    @pl.when(sp == 0)
    def _():
        edge_in[0] = jnp.zeros(edge_in.shape[1:], F32)

    @pl.when(sp == n - 1)
    def _():
        edge_in[1] = jnp.zeros(edge_in.shape[1:], F32)

    barrier = pltpu.get_barrier_semaphore()
    sp_peer = [lax.rem(sp + k, n) for k in range(1, n)]
    tp_peer = [lax.rem(tp + k, tps) for k in range(1, tps)]
    dp_peer = [lax.rem(dp + k, dps) for k in range(1, dps)]
    place_peer = []
    for a in range(tps):
        for b in range(dps):
            if a or b:
                place_peer.append((lax.rem(tp + a, tps), lax.rem(dp + b, dps)))
    for p in sp_peer:
        pl.semaphore_signal(barrier, inc=1, device_id={"sp": p}, device_id_type=MESH)
    for a, b in place_peer:
        pl.semaphore_signal(barrier, inc=1, device_id={"tp": a, "dp": b}, device_id_type=MESH)
    sends = []

    def send(src, dst, ssem, rsem, dev):
        c = pltpu.make_async_remote_copy(
            src_ref=src, dst_ref=dst, send_sem=ssem, recv_sem=rsem,
            device_id=dev, device_id_type=MESH,
        )
        c.start()
        return c

    def arrived(dst, rsem):
        pltpu.make_async_copy(dst, dst, rsem).wait()

    act[...] = jnp.zeros(act.shape, F32)
    act[0:1, :] = silu(cond[...].astype(F32)).astype(BF16).astype(F32).reshape(1, -1)
    act[1:2, :] = silu(ctx_cond[...].astype(F32)).astype(BF16).astype(F32).reshape(1, -1)
    own_act = act[:, pl.ds(pl.multiple_of(sp * mod_rows, 128), mod_rows)].astype(BF16)
    ld_shift.wait()
    mod_part[0:2, :] = dot(own_act, mod_w[0])[0:2]
    ld_scale.wait()
    mod_part[2:4, :] = dot(own_act, mod_w[1])[0:2]
    ld_lat = load(latent, lat_v.at[pl.ds(dp * half, half)])
    ld_ctx = load(context, ctx_v)
    ld_gatew = load(gate_w, mod_w.at[0])
    ld_sig = load(w_sig, w_all.at[:, pl.ds(sw, inner)])
    ld_wr = load(w_wr, w_all.at[:, pl.ds(0, sw)])
    ld_st = load(w_step, w_st)
    ld_rd = load(w_rd, w_all.at[:, pl.ds(inner + sw, sw)])
    ld_gate = load(w_gate, w_all.at[:, pl.ds(inner + 2 * sw, inner)])
    ld_outs = [
        load(w_out.at[pl.ds(q * inner + g * gw, gw)], w_o.at[g, pl.ds(q * gw, gw)])
        for g in range(group_count) for q in range(places)
    ]
    pl.semaphore_wait(barrier, len(sp_peer) + len(place_peer))
    for k, p in enumerate(sp_peer):
        sends.append(send(mod_part, mod_in.at[sp], mod_sem.at[0, k], mod_sem.at[1, sp], {"sp": p}))
    mod_in[sp] = mod_part[...]

    for k, p in enumerate(dp_peer):
        sends.append(send(latent, lat_v.at[pl.ds(dp * half, half)], lat_sem.at[0, k],
                          lat_sem.at[1, dp], {"dp": p}))

    def inv_rms(v):
        return lax.rsqrt(jnp.mean(v * v, axis=-1, keepdims=True) + EPSILON)

    lat_rms, ctx_rms = slice(0, 128), slice(128, 256)

    def row_tile(rows):
        return min(rows, 64)

    def rms_rows(ref, keep, start, count):
        tile = row_tile(count)

        def step(t, carry):
            at = pl.ds(pl.multiple_of(start + t * tile, tile), tile)
            total = jnp.zeros((tile, 128), F32)
            for c in range(width // 128):
                v = ref[at, c * 128:(c + 1) * 128].astype(F32)
                total = total + v * v
            mean = jnp.sum(total, axis=-1, keepdims=True) * (1.0 / width)
            in_block[at, keep] = jnp.broadcast_to(lax.rsqrt(mean + EPSILON), (tile, 128))
            return carry

        lax.fori_loop(0, count // tile, step, 0)

    ld_lat.wait()
    rms_rows(lat_v, lat_rms, dp * half, half)

    for p in sp_peer:
        arrived(mod_in.at[p], mod_sem.at[1, p])
    total = mod_in[0]
    for q in range(1, n):
        total = total + mod_in[q]
    mod_sum[...] = total
    for k, (a, b) in enumerate(place_peer):
        sends.append(send(mod_sum, mod_all.at[place], mod_sem.at[4, k], mod_sem.at[5, place],
                          {"tp": a, "dp": b}))
    mod_all[place] = total

    ld_ctx.wait()
    for p in dp_peer:
        arrived(lat_v.at[pl.ds(p * half, half)], lat_sem.at[1, p])
    pieces = width // 128
    first_lat = lat_v[0:16, :].astype(F32)[0:1]
    last_lat = lat_v[length - 16:length, :].astype(F32)[15:16]
    first_ctx = ctx_v[0:16, :].astype(F32)[0:1]
    last_ctx = ctx_v[ctx_len - 16:ctx_len, :].astype(F32)[15:16]
    for i in range(pieces):
        cols = slice(i * 128, (i + 1) * 128)
        edge_out[0, 0, i:i + 1, :] = last_lat[:, cols]
        edge_out[0, 1, i:i + 1, :] = last_ctx[:, cols]
        edge_out[1, 0, i:i + 1, :] = first_lat[:, cols]
        edge_out[1, 1, i:i + 1, :] = first_ctx[:, cols]

    def edge_copy(side):
        dev = sp + 1 if side == 0 else sp - 1
        return pltpu.make_async_remote_copy(
            src_ref=edge_out.at[side], dst_ref=edge_in.at[side], send_sem=edge_sem.at[0, side],
            recv_sem=edge_sem.at[1, side], device_id={"sp": dev}, device_id_type=MESH)

    @pl.when(sp < n - 1)
    def _():
        edge_copy(0).start()

    @pl.when(sp > 0)
    def _():
        edge_copy(1).start()

    for p in dp_peer:
        rms_rows(lat_v, lat_rms, p * half, half)
    rms_rows(ctx_v, ctx_rms, 0, ctx_len)
    own_out = pl.ds(pl.multiple_of(place * out_cols, 128), out_cols)

    def keep_rows(b, carry):
        at = pl.ds(pl.multiple_of(b * BLOCK, BLOCK), BLOCK)
        out[at, :] = lat_v[at, own_out]
        return carry

    lax.fori_loop(0, blocks, keep_rows, 0)
    ld_gatew.wait()
    gate_part[...] = dot(own_act, mod_w[0])[0:1]
    for k, p in enumerate(sp_peer):
        sends.append(send(gate_part, gate_in.at[sp], mod_sem.at[2, k], mod_sem.at[3, sp], {"sp": p}))
    gate_in[sp] = gate_part[...]

    low_r = lax.broadcasted_iota(jnp.int32, (BLOCK, BLOCK), 0)
    low_c = lax.broadcasted_iota(jnp.int32, (BLOCK, BLOCK), 1)
    lanes2 = 2 * heads
    er = lax.broadcasted_iota(jnp.int32, (lanes2, lanes2 * head_dim), 0)
    ec = lax.broadcasted_iota(jnp.int32, (lanes2, lanes2 * head_dim), 1)
    one = ((ec >= er * head_dim) & (ec < (er + 1) * head_dim)).astype(F32)
    spread[...] = jnp.concatenate([one, one, one], axis=0).astype(BF16)

    def widen(v):
        return jnp.concatenate(thirds(v), axis=1)

    for a, b in place_peer:
        arrived(mod_all.at[a * dps + b], mod_sem.at[5, a * dps + b])
    for j in range(places):
        cols = slice(j * mod_cols, (j + 1) * mod_cols)
        block_mod = mod_all[j]
        g = gain[0:1, cols]
        for r in range(2):
            shift_rows[r, :, cols] = jnp.broadcast_to(block_mod[r:r + 1], (8, mod_cols))
            scale_rows[r, :, cols] = jnp.broadcast_to((1.0 + block_mod[2 + r:3 + r]) * g, (8, mod_cols))

    def hidden_rows(ref, keep, goal, which, start, count):
        tile = row_tile(count)

        def step(t, carry):
            at = pl.ds(pl.multiple_of(start + t * tile, tile), tile)
            r3 = in_block[at, keep].reshape(tile // 8, 8, 128)
            for c in range(width // 128):
                cols = slice(c * 128, (c + 1) * 128)
                v = ref[at, cols].astype(F32).reshape(tile // 8, 8, 128)
                h = v * r3 * scale_rows[which, :, cols][None] + shift_rows[which, :, cols][None]
                goal[at, cols] = h.reshape(tile, 128).astype(BF16)
            return carry

        lax.fori_loop(0, count // tile, step, 0)

    hidden_rows(ctx_v, ctx_rms, hid_c, 1, 0, ctx_len)

    @pl.when(sp > 0)
    def _():
        arrived(edge_in.at[0], edge_sem.at[1, 0])

    @pl.when(sp < n - 1)
    def _():
        arrived(edge_in.at[1], edge_sem.at[1, 1])

    edge_rows[...] = jnp.zeros(edge_rows.shape, F32)
    for i in range(pieces):
        cols = slice(i * 128, (i + 1) * 128)
        edge_rows[0:1, cols] = edge_in[0, 0, i:i + 1, :]
        edge_rows[1:2, cols] = edge_in[1, 0, i:i + 1, :]
        edge_rows[2:3, cols] = edge_in[0, 1, i:i + 1, :]
        edge_rows[3:4, cols] = edge_in[1, 1, i:i + 1, :]
    edge_v = edge_rows[...]
    edge_n = edge_v * inv_rms(edge_v)
    is_lat = lax.broadcasted_iota(jnp.int32, edge_v.shape, 0) < 2
    edge_hid = jnp.where(is_lat, edge_n * scale_rows[0] + shift_rows[0],
                         edge_n * scale_rows[1] + shift_rows[1])
    hid_c[ctx_len:ctx_len + 16, :] = jnp.concatenate([edge_hid, jnp.zeros_like(edge_hid)], axis=0).astype(BF16)

    ld_sig.wait()
    ld_wr.wait()
    ld_rd.wait()
    has_above = (sp > 0).astype(F32)
    has_below = (sp < n - 1).astype(F32)

    def ctx_proj(t, carry):
        cols = pl.ds(pl.multiple_of(t * TILE_N, TILE_N), TILE_N)
        got = dot(hid_c[...], w_all[:, cols]).astype(BF16).astype(F32)
        for i in range(TILE_N // 128):
            c, piece = t * (TILE_N // 128) + i, got[:, i * 128:(i + 1) * 128]
            raw_c[c, 8:8 + ctx_len, :] = piece[0:ctx_len]
            edges = piece[ctx_len:ctx_len + 8]
            raw[c, 0:8, :] = jnp.broadcast_to(edges[0:1] * has_above, (8, 128))
            raw[c, 8 + length:16 + length, :] = jnp.broadcast_to(edges[1:2] * has_below, (8, 128))
            raw_c[c, 0:8, :] = jnp.broadcast_to(edges[2:3] * has_above, (8, 128))
            raw_c[c, 8 + ctx_len:16 + ctx_len, :] = jnp.broadcast_to(edges[3:4] * has_below, (8, 128))
        return carry

    lax.fori_loop(0, (inner + 2 * sw) // TILE_N, ctx_proj, 0)
    ld_st.wait()
    ctx_step_in = dot_t(hid_c[0:ctx_len], w_st[...]).astype(BF16).astype(F32)

    bias = jnp.concatenate([step_bias[0:1], step_bias[1:2]], axis=1)
    rates = -jnp.exp(jnp.concatenate([decay_log[0:1], decay_log[1:2]], axis=1))

    def sums(ld, size):
        r = lax.broadcasted_iota(jnp.int32, (size, size), 0)
        c = lax.broadcasted_iota(jnp.int32, (size, size), 1)
        tri = jnp.concatenate([(r >= c).astype(F32), (r <= c).astype(F32)], axis=0).astype(BF16)
        parts = thirds(ld)
        both = dot(tri, parts[0]) + (dot(tri, parts[1]) + dot(tri, parts[2]))
        lane = lax.broadcasted_iota(jnp.int32, (1, ld.shape[1]), 1)
        forward = lax.rem(lane, lanes2) < heads
        cum = jnp.where(forward, both[:size], both[size:])
        return cum, jnp.where(forward, cum[size - 1:size], cum[0:1])

    def conv(ref, taps, first, start, count, cols, size):
        outs = []
        for i in range(count):
            tc = slice(cols + i * 128, cols + (i + 1) * 128)
            v = (taps[0:1, tc] * ref[first + i, pl.ds(start + 7, size), :]
                 + taps[1:2, tc] * ref[first + i, pl.ds(start + 8, size), :]
                 + taps[2:3, tc] * ref[first + i, pl.ds(start + 9, size), :])
            outs.append(silu(v))
        return outs[0] if count == 1 else jnp.concatenate(outs, axis=1)

    gp, sig_first, rd_first = gw // 128, sw // 128, (inner + sw) // 128

    def widened(v, cols):
        return dot(widen(v), spread[:, cols])

    def span_states(sig_g, wr_g, w_f, w_b):
        rhs = jnp.concatenate([sig_g * w_f, sig_g * w_b], axis=1).astype(BF16)
        return lax.dot_general(wr_g, rhs, (((0,), (0,)), ((), ())), preferred_element_type=F32)

    def group_cols(side, g):
        return slice(side * inner + g * gw, side * inner + (g + 1) * gw)

    ctx_step = softplus(ctx_step_in + bias)
    ctx_cum, ctx_end = sums(rates * ctx_step, ctx_len)
    ctx_w = widen(jnp.exp(ctx_end - ctx_cum) * ctx_step)
    ctx_dec8 = widened(jnp.broadcast_to(jnp.exp(ctx_end), (8, lanes2)), slice(0, 2 * inner))
    for g in range(group_count):
        sig_g = conv(raw_c, sig_taps, sig_first + g * gp, 0, gp, g * gw, ctx_len)
        wr_g = conv(raw_c, wr_taps, g, 0, 1, g * STATE, ctx_len).astype(BF16)
        got = span_states(sig_g, wr_g, dot(ctx_w, spread[:, group_cols(0, g)]),
                          dot(ctx_w, spread[:, group_cols(1, g)]))
        ctx_acc[0, g] = got[:, :gw]
        ctx_acc[1, g] = got[:, gw:]

    firsts = (0, n - 1)

    def ctx_copy(side, part):
        if part < group_count:
            src, dst = ctx_send.at[side, part], ctx_recv.at[side, sp, part]
        else:
            src, dst = cdec_send.at[side], cdec_recv.at[side, sp]
        return pltpu.make_async_remote_copy(
            src_ref=src, dst_ref=dst, send_sem=cchain_sem.at[0, side, 0, part],
            recv_sem=cchain_sem.at[1, side, sp, part], device_id={"sp": firsts[side]},
            device_id_type=MESH)

    for side in range(2):
        cdec_send[side] = ctx_dec8[0:1, side * inner:(side + 1) * inner]
        ctx_send[side] = ctx_acc[side].astype(BF16)
    for part in [group_count] + list(range(group_count)):
        for side in range(2):
            @pl.when(sp != firsts[side])
            def _():
                ctx_copy(side, part).start()

    def ctx_collect(side, g):
        for d in range(1, n):
            q = d if side == 0 else n - 1 - d
            if g == 0:
                arrived(cdec_recv.at[side, q], cchain_sem.at[1, side, q, group_count])
            arrived(ctx_recv.at[side, q, g], cchain_sem.at[1, side, q, g])
            ctx_acc[side, g] = (ctx_acc[side, g] * cdec_recv[side, q, :, g * gw:(g + 1) * gw]
                                + ctx_recv[side, q, g].astype(F32))

    hidden_rows(lat_v, lat_rms, lat_v, 0, 0, length)
    st_raw = dot_t(lat_v[...], w_st[...]).astype(BF16).astype(F32)

    def by_block(v):
        return jnp.concatenate([v] * blocks, axis=1)

    step = softplus(jnp.concatenate([st_raw[b * BLOCK:(b + 1) * BLOCK] for b in range(blocks)], axis=1)
                    + by_block(bias))
    more = jnp.concatenate([extra[:, b * BLOCK:(b + 1) * BLOCK] for b in range(blocks)], axis=0).T
    cum, end = sums(by_block(rates) * step + more, BLOCK)
    weight, grow = jnp.exp(end - cum) * step, jnp.exp(cum)
    cum_t, step_t = cum.T, step.T
    ends = jnp.exp(end)
    for b in range(blocks):
        at_b = slice(b * lanes2, (b + 1) * lanes2)
        cum_col[b] = cum[:, at_b]
        ecum_col[b] = widen(grow[:, at_b])
        weight_col[b] = widen(weight[:, at_b])
        cum_row[b] = cum_t[at_b]
        step_row[b] = step_t[at_b]
        dec[b] = widened(jnp.broadcast_to(ends[:, at_b], (8, lanes2)), slice(0, 2 * inner))
    dec_all = dec[0]
    for b in range(1, blocks):
        dec_all = dec_all * dec[b]
    for side in range(2):
        sdec_send[side] = dec_all[0:1, side * inner:(side + 1) * inner]

    def chain_copy(side, d, part):
        if part < group_count:
            src, dst = chain_out.at[side, part], chain_recv.at[side, sp, part]
        else:
            src, dst = sdec_send.at[side], sdec_recv.at[side, sp]
        return pltpu.make_async_remote_copy(
            src_ref=src, dst_ref=dst, send_sem=chain_sem.at[0, side, d, part],
            recv_sem=chain_sem.at[1, side, sp, part],
            device_id={"sp": sp + d if side == 0 else sp - d}, device_id_type=MESH)

    def has_goal(side, d):
        return sp + d < n if side == 0 else sp - d >= 0

    def is_source(side, q):
        return sp > q if side == 0 else sp < q

    for d in range(n - 1, 0, -1):
        for side in range(2):
            @pl.when(has_goal(side, d) & (sp != firsts[side]))
            def _():
                chain_copy(side, d, group_count).start()

    def chain_start(g):
        for side in range(2):
            @pl.when(sp == firsts[side])
            def _():
                ctx_collect(side, g)
                if n > 1:
                    chain_out[side, g] = (ctx_acc[side, g] * dec_all[0:1, group_cols(side, g)]
                                          + span_total[side, g]).astype(BF16)

            @pl.when(sp != firsts[side])
            def _():
                chain_out[side, g] = span_total[side, g].astype(BF16)
        for d in range(n - 1, 0, -1):
            for side in range(2):
                @pl.when(has_goal(side, d))
                def _():
                    chain_copy(side, d, g).start()

    def chain_end(g):
        for side in range(2):
            @pl.when(sp == firsts[side])
            def _():
                chain_in[side, g] = ctx_acc[side, g]

            if n > 1:
                @pl.when(sp != firsts[side])
                def _():
                    arrived(chain_recv.at[side, firsts[side], g], chain_sem.at[1, side, firsts[side], g])
                    chain_in[side, g] = chain_recv[side, firsts[side], g].astype(F32)

            for d in range(1, n - 1):
                q = d if side == 0 else n - 1 - d

                @pl.when(is_source(side, q))
                def _():
                    if g == 0:
                        arrived(sdec_recv.at[side, q], chain_sem.at[1, side, q, group_count])
                    arrived(chain_recv.at[side, q, g], chain_sem.at[1, side, q, g])
                    chain_in[side, g] = (
                        chain_in[side, g] * sdec_recv[side, q, :, g * gw:(g + 1) * gw]
                        + chain_recv[side, q, g].astype(F32))

    def hidden_dot(first, size):
        if size % 512 == 0:
            return dot(lat_v[...], w_all[:, first:first + size])
        near = dot(lat_v[:, :width // 2], w_all[:width // 2, first:first + size])
        return near + dot(lat_v[:, width // 2:], w_all[width // 2:, first:first + size])

    def project(first, size):
        got = hidden_dot(first, size).astype(BF16).astype(F32)
        for i in range(size // 128):
            raw[first // 128 + i, 8:8 + length, :] = got[:, i * 128:(i + 1) * 128]

    def gate_project(g):
        gates[:, g * gw:(g + 1) * gw] = hidden_dot(inner + 2 * sw + g * gw, gw).astype(BF16)

    def block_at(side, i):
        return i if side == 0 else blocks - 1 - i

    def side_cols(side):
        return slice(side * gw, (side + 1) * gw)

    def group_states(g):
        gc = slice(g * gw, (g + 1) * gw)

        def step(b, carry):
            start = pl.multiple_of(b * BLOCK, BLOCK)
            at = pl.ds(start, BLOCK)
            sig_g = conv(raw, sig_taps, sig_first + g * gp, start, gp, g * gw, BLOCK)
            wr_g = conv(raw, wr_taps, g, start, 1, g * STATE, BLOCK).astype(BF16)
            sig[at, gc] = sig_g.astype(BF16)
            wr[at, g * STATE:(g + 1) * STATE] = wr_g
            wide = weight_col[b]
            states[b, g] = span_states(sig_g, wr_g, dot(wide, spread[:, group_cols(0, g)]),
                                       dot(wide, spread[:, group_cols(1, g)]))
            return carry

        lax.fori_loop(0, blocks, step, 0, unroll=2)
        for side in range(2):
            def total_step(i, run):
                b = block_at(side, i)
                return run * dec[b, 0:1, group_cols(side, g)] + states[b, g, :, side_cols(side)]

            span_total[side, g] = lax.fori_loop(0, blocks, total_step, jnp.zeros((STATE, gw), F32))

    def group_blocks(g):
        gc = slice(g * gw, (g + 1) * gw)

        def step(b, carry):
            start = pl.multiple_of(b * BLOCK, BLOCK)
            at = pl.ds(start, BLOCK)
            cr, sr, cc = cum_row[b], step_row[b], cum_col[b]
            lane_g = lax.broadcasted_iota(jnp.int32, (BLOCK, gw), 1)
            rd_g = conv(raw, rd_taps, rd_first + g, start, 1, g * STATE, BLOCK).astype(BF16)
            rd[at, g * STATE:(g + 1) * STATE] = rd_g
            wr_g = wr[at, g * STATE:(g + 1) * STATE]
            sig_g = sig[at, gc]
            pair = dot_t(rd_g, wr_g)
            mixes, sigs = [], []
            for e in range(per_group):
                f, k = g * per_group + e, heads + g * per_group + e
                gap = jnp.where(low_r >= low_c, cc[:, f:f + 1] - cr[f:f + 1], cc[:, k:k + 1] - cr[k:k + 1])
                sf, sk = sr[f:f + 1], sr[k:k + 1]
                size = jnp.where(low_r > low_c, sf, jnp.where(low_r < low_c, sk, sf + sk))
                mixes.append((jnp.exp(gap) * size * pair).astype(BF16))
                mine = (lane_g >= e * head_dim) & (lane_g < (e + 1) * head_dim)
                sigs.append(jnp.where(mine, sig_g, jnp.zeros_like(sig_g)))
            in_block[at, gc] = dot(jnp.concatenate(mixes, axis=1), jnp.concatenate(sigs, axis=0))
            return carry

        lax.fori_loop(0, blocks, step, 0, unroll=2)

    chunk = pl.ds(pl.multiple_of(place * gw, 128), gw)

    def norm_copy(g, b, cols, dev, slot, sender):
        ref = normed.at[g, pl.ds(pl.multiple_of(b * BLOCK, BLOCK), BLOCK), cols]
        return pltpu.make_async_remote_copy(
            src_ref=ref, dst_ref=ref, send_sem=norm_sem.at[0, slot, g, b],
            recv_sem=norm_sem.at[1, sender, g, b], device_id=dev, device_id_type=MESH)

    def place_cols(q):
        return pl.ds(pl.multiple_of(q * gw, 128), gw)

    def finish_group(g):
        gc = slice(g * gw, (g + 1) * gw)
        for side in range(2):
            def enter(i, run):
                b = block_at(side, i)
                ent[b, g, :, side_cols(side)] = run.astype(BF16)
                return run * dec[b, 0:1, group_cols(side, g)] + states[b, g, :, side_cols(side)]

            lax.fori_loop(0, blocks, enter, chain_in[side, g])

        def finish(b, carry):
            at = pl.ds(pl.multiple_of(b * BLOCK, BLOCK), BLOCK)
            carried = dot(rd[at, g * STATE:(g + 1) * STATE], ent[b, g])
            grown = ecum_col[b]
            both = (in_block[at, gc]
                    + carried[:, :gw] * dot(grown, spread[:, group_cols(0, g)])
                    + carried[:, gw:] * dot(grown, spread[:, group_cols(1, g)]))
            gated = both * silu(gates[at, gc].astype(F32))
            done = gated * inv_rms(gated) * group_gain[0:1, gc]
            normed[g, at, chunk] = done.astype(BF16)
            for k, a in enumerate(tp_peer):
                norm_copy(g, b, chunk, {"tp": a}, k, place).start()
            for k, p in enumerate(dp_peer):
                norm_copy(g, b, chunk, {"dp": p}, tps - 1 + k, place).start()
            return carry

        lax.fori_loop(0, blocks, finish, 0)

    project(0, sw + gw)
    group_states(0)
    chain_start(0)
    for g in range(1, group_count):
        project(sw + g * gw, gw)
        group_states(g)
    project(sw + inner, sw)
    for g in range(1, group_count):
        chain_start(g)
    ld_gate.wait()
    for g in range(group_count):
        group_blocks(g)
        gate_project(g)
        chain_end(g)
        finish_group(g)

    for p in sp_peer:
        arrived(gate_in.at[p], mod_sem.at[3, p])
    gate_vec = gate_in[0]
    for q in range(1, n):
        gate_vec = gate_vec + gate_in[q]

    for c in ld_outs:
        c.wait()
    slots = (tps - 1) + (dps - 1)

    def relay(g, b):
        for k, a in enumerate(tp_peer):
            q = a * dps + dp
            norm_copy(g, b, place_cols(q), {"tp": a}, 0, q).wait_recv()
            for j, p in enumerate(dp_peer):
                slot = slots + k * (dps - 1) + j
                norm_copy(g, b, place_cols(q), {"dp": p}, slot, q).start()

    def gathered(g, b):
        for p in dp_peer:
            for a in range(tps):
                q = a * dps + p
                norm_copy(g, b, place_cols(q), {"dp": p}, 0, q).wait_recv()

    def held(b):
        return jnp.concatenate([states[b, j] for j in range(group_count)], axis=1)

    for g in range(group_count - 1):
        lax.fori_loop(0, blocks, lambda b, carry: (relay(g, b), carry)[1], 0)
        lax.fori_loop(0, blocks, lambda b, carry: (gathered(g, b), carry)[1], 0)
        part = dot(normed[g], w_o[g])
        for b in range(blocks):
            piece = part[b * BLOCK:(b + 1) * BLOCK]
            if g > 0:
                piece = piece + held(b)
            for j in range(group_count):
                states[b, j] = piece[:, j * 2 * gw:(j + 1) * 2 * gw]

    def finished(first, count):
        g = group_count - 1
        for b in range(first, first + count):
            gathered(g, b)
        at = pl.ds(first * BLOCK, count * BLOCK)
        part = dot(normed[g, at, :], w_o[g])
        if g > 0:
            part = part + jnp.concatenate([held(b) for b in range(first, first + count)], axis=0)
        out[at, :] = (out[at, :].astype(F32) + gate_vec * part).astype(BF16)

    spans, first = [], 0
    while first < blocks:
        count = 2 if blocks - first > 2 else 1
        spans.append((first, count))
        first += count
    for i, (first, count) in enumerate(spans):
        for b in range(first, first + count):
            relay(group_count - 1, b)
        if i > 0:
            finished(*spans[i - 1])
    finished(*spans[-1])

    for c in sends:
        c.wait_send()

    @pl.when(sp < n - 1)
    def _():
        edge_copy(0).wait_send()

    @pl.when(sp > 0)
    def _():
        edge_copy(1).wait_send()

    for side in range(2):
        @pl.when(sp != firsts[side])
        def _():
            for part in range(group_count + 1):
                ctx_copy(side, part).wait_send()

        for d in range(1, n):
            @pl.when(has_goal(side, d))
            def _():
                for g in range(group_count):
                    chain_copy(side, d, g).wait_send()

            @pl.when(has_goal(side, d) & (sp != firsts[side]))
            def _():
                chain_copy(side, d, group_count).wait_send()

    for g in range(group_count):
        def drained(b, carry):
            for k, a in enumerate(tp_peer):
                norm_copy(g, b, chunk, {"tp": a}, k, place).wait_send()
            for k, p in enumerate(dp_peer):
                norm_copy(g, b, chunk, {"dp": p}, tps - 1 + k, place).wait_send()
            for k, a in enumerate(tp_peer):
                for j, p in enumerate(dp_peer):
                    slot = slots + k * (dps - 1) + j
                    norm_copy(g, b, place_cols(a * dps + dp), {"dp": p}, slot, place).wait_send()
            return carry

        lax.fori_loop(0, blocks, drained, 0)


def on_device(dims, *args):
    (
        latent, context, condition, context_condition, shift_weight, scale_weight, gate_weight,
        norm_gain, out_gate_weight, signal_weight, writer_weight, reader_matrix, step_weight,
        signal_taps, writer_taps, reader_taps, step_bias, decay_log, decay_extra, group_gain,
        output_weight,
    ) = args
    n, tps, dps = dims
    half, width = latent.shape
    length = half * dps
    ctx_len = context.shape[0]
    heads = step_bias.shape[1]
    inner = signal_weight.shape[1]
    sw = writer_weight.shape[1]
    groups = sw // STATE
    gw = inner // groups
    blocks = length // BLOCK
    places = tps * dps
    mod_rows, mod_cols = shift_weight.shape
    out_cols = output_weight.shape[1]
    lanes2 = 2 * heads
    conv_cols = inner + 2 * sw
    steps = jnp.swapaxes(step_weight, 1, 2).reshape(lanes2, width)
    hbm = pl.BlockSpec(memory_space=pltpu.HBM)
    vmem = pl.BlockSpec(memory_space=pltpu.VMEM)
    slots = (tps - 1) + (dps - 1) + (tps - 1) * (dps - 1)
    peers = max(n - 1, places - 1, 1)
    scratch = [
        pltpu.VMEM((length, width), BF16),
        pltpu.VMEM((ctx_len, width), BF16),
        pltpu.VMEM((8, width), F32),
        pltpu.VMEM((2, mod_rows, mod_cols), BF16),
        pltpu.VMEM((4, mod_cols), F32),
        pltpu.VMEM((1, mod_cols), F32),
        pltpu.VMEM((n, 4, mod_cols), F32),
        pltpu.VMEM((n, 1, mod_cols), F32),
        pltpu.VMEM((4, mod_cols), F32),
        pltpu.VMEM((places, 4, mod_cols), F32),
        pltpu.VMEM((2, 8, width), F32),
        pltpu.VMEM((2, 8, width), F32),
        pltpu.VMEM((2, 2, width // 128, 128), F32),
        pltpu.VMEM((2, 2, width // 128, 128), F32),
        pltpu.VMEM((8, width), F32),
        pltpu.VMEM((ctx_len + 16, width), BF16),
        pltpu.VMEM((width, 2 * inner + 2 * sw), BF16),
        pltpu.VMEM((lanes2, width), BF16),
        pltpu.VMEM((groups, places * gw, out_cols), BF16),
        pltpu.VMEM((conv_cols // 128, length + 16, 128), F32),
        pltpu.VMEM((conv_cols // 128, ctx_len + 16, 128), F32),
        pltpu.VMEM((length, inner), BF16),
        pltpu.VMEM((blocks, BLOCK, lanes2), F32),
        pltpu.VMEM((blocks, BLOCK, 3 * lanes2), BF16),
        pltpu.VMEM((blocks, BLOCK, 3 * lanes2), BF16),
        pltpu.VMEM((blocks, lanes2, BLOCK), F32),
        pltpu.VMEM((blocks, lanes2, BLOCK), F32),
        pltpu.VMEM((length, inner), BF16),
        pltpu.VMEM((length, sw), BF16),
        pltpu.VMEM((length, sw), BF16),
        pltpu.VMEM((blocks, groups, STATE, 2 * gw), F32),
        pltpu.VMEM((blocks, 8, 2 * inner), F32),
        pltpu.VMEM((blocks, groups, STATE, 2 * gw), BF16),
        pltpu.VMEM((2, groups, STATE, gw), F32),
        pltpu.VMEM((2, groups, STATE, gw), BF16),
        pltpu.VMEM((2, n, groups, STATE, gw), BF16),
        pltpu.VMEM((2, 1, inner), F32),
        pltpu.VMEM((2, n, 1, inner), F32),
        pltpu.VMEM((2, 1, inner), F32),
        pltpu.VMEM((2, n, 1, inner), F32),
        pltpu.VMEM((2, groups, STATE, gw), F32),
        pltpu.VMEM((2, groups, STATE, gw), BF16),
        pltpu.VMEM((2, n, groups, STATE, gw), BF16),
        pltpu.VMEM((2, groups, STATE, gw), F32),
        pltpu.VMEM((3 * lanes2, 2 * inner), BF16),
        pltpu.VMEM((length, inner), F32),
        pltpu.VMEM((groups, length, places * gw), BF16),
        pltpu.SemaphoreType.DMA((10 + groups * places,)),
        pltpu.SemaphoreType.DMA((2, dps)),
        pltpu.SemaphoreType.DMA((6, max(n, places))),
        pltpu.SemaphoreType.DMA((2, 2)),
        pltpu.SemaphoreType.DMA((2, 2, n, groups + 1)),
        pltpu.SemaphoreType.DMA((2, 2, n, groups + 1)),
        pltpu.SemaphoreType.DMA((2, max(slots, places), groups, blocks)),
    ]
    specs = [hbm, hbm, vmem, vmem, hbm, hbm, hbm, vmem, hbm, hbm, hbm, hbm, hbm,
             vmem, vmem, vmem, vmem, vmem, vmem, vmem, hbm]
    operands = (
        latent, context, condition, context_condition, shift_weight, scale_weight, gate_weight,
        norm_gain.reshape(1, -1), out_gate_weight, signal_weight, writer_weight, reader_matrix,
        steps, signal_taps, writer_taps, reader_taps, step_bias, decay_log,
        decay_extra.reshape(lanes2, length), group_gain.reshape(1, -1), output_weight,
    )
    return pl.pallas_call(
        functools.partial(kernel, dims),
        out_shape=pltpu.VMEM((length, out_cols), BF16),
        in_specs=specs,
        out_specs=vmem,
        scratch_shapes=scratch,
        compiler_params=pltpu.CompilerParams(
            collective_id=0, has_side_effects=True, vmem_limit_bytes=60000000),
    )(*[pltpu.with_memory_space_constraint(x, pltpu.HBM) for x in operands])


def solution(mesh):
    dims = (mesh.shape["sp"], mesh.shape["tp"], mesh.shape["dp"])
    in_specs = (
        P(("grp", "sp", "dp"), None),
        P(("grp", "sp"), None),
        P("grp"),
        P(),
        P("sp", ("tp", "dp")),
        P("sp", ("tp", "dp")),
        P("sp", ("tp", "dp")),
        P(),
        P(None, ("tp", "dp")),
        P(None, ("tp", "dp")),
        P(None, ("tp", "dp")),
        P(None, ("tp", "dp")),
        P(None, None, ("tp", "dp")),
        P(None, ("tp", "dp")),
        P(None, ("tp", "dp")),
        P(None, ("tp", "dp")),
        P(None, ("tp", "dp")),
        P(None, ("tp", "dp")),
        P(None, ("tp", "dp"), ("grp", "sp")),
        P(("tp", "dp")),
        P(None, ("tp", "dp")),
    )
    out_specs = P(("grp", "sp"), ("tp", "dp"))
    return jax.shard_map(
        functools.partial(on_device, dims), mesh=mesh, in_specs=in_specs, out_specs=out_specs,
        check_vma=False,
    )
```

```python
import functools

import jax
import jax.numpy as jnp
from jax import lax
from jax.experimental import pallas as pl
from jax.experimental.pallas import tpu as pltpu
from jax.sharding import PartitionSpec as P

STATE = 128
BLOCK = 128
EPSILON = 1e-06
TILE_N = 512
F32 = jnp.float32
BF16 = jnp.bfloat16
MESH = pl.DeviceIdType.MESH


def silu(v):
    return v / (1.0 + jnp.exp(-v))


def softplus(v):
    return jnp.maximum(v, 0.0) + jnp.log1p(jnp.exp(-jnp.abs(v)))


def dot(a, b):
    return jnp.dot(a, b, preferred_element_type=F32)


def dot_t(a, b):
    return lax.dot_general(a, b, (((1,), (1,)), ((), ())), preferred_element_type=F32)


def thirds(v):
    first = v.astype(BF16)
    rest = v - first.astype(F32)
    second = rest.astype(BF16)
    third = (rest - second.astype(F32)).astype(BF16)
    return first, second, third


def kernel(dims, *refs):
    (
        latent, context, cond_h, ctx_cond_h, shift_w, scale_w, gate_w, gain_h,
        w_gate, w_sig, w_wr, w_rd, w_step, sig_taps_h, wr_taps_h, rd_taps_h, step_bias_h, decay_log_h,
        extra_h, group_gain_h, w_out, out,
        cond, ctx_cond, gain, sig_taps, wr_taps, rd_taps, step_bias, decay_log, extra, group_gain,
        lat_v, ctx_v, act, mod_w, mod_part, gate_part, mod_in, gate_in, mod_sum, mod_all,
        scale_rows, shift_rows, edge_out, edge_in, edge_rows, hid_c, w_all, w_st, w_o,
        raw, raw_c, gates, cum_col, ecum_col, weight_col, cum_row, step_row, sig, wr, rd,
        states, dec, ent, ctx_acc, ctx_send, ctx_recv, cdec_send, cdec_recv, sdec_send, sdec_recv,
        span_total, chain_out, chain_recv, chain_in, spread, in_block, normed,
        load_sem, lat_sem, mod_sem, edge_sem, cchain_sem, chain_sem, norm_sem,
    ) = refs
    n, tps, dps = dims
    sp, tp, dp = lax.axis_index("sp"), lax.axis_index("tp"), lax.axis_index("dp")
    place = tp * dps + dp
    places = tps * dps
    width = latent.shape[1]
    half = latent.shape[0]
    length = lat_v.shape[0]
    ctx_len = context.shape[0]
    heads = step_bias.shape[1]
    inner = w_sig.shape[1]
    head_dim = inner // heads
    group_count = w_wr.shape[1] // STATE
    per_group = heads // group_count
    gw = per_group * head_dim
    sw = w_wr.shape[1]
    blocks = length // BLOCK
    mod_rows, mod_cols = shift_w.shape
    out_cols = out.shape[1]

    loads = []

    def load(src, dst):
        c = pltpu.make_async_copy(src, dst, load_sem.at[len(loads)])
        c.start()
        loads.append(c)
        return c

    ld_conds = [load(cond_h, cond), load(ctx_cond_h, ctx_cond)]
    ld_shift = load(shift_w, mod_w.at[0])
    ld_scale = load(scale_w, mod_w.at[1])

    @pl.when(sp == 0)
    def _():
        edge_in[0] = jnp.zeros(edge_in.shape[1:], F32)

    @pl.when(sp == n - 1)
    def _():
        edge_in[1] = jnp.zeros(edge_in.shape[1:], F32)

    barrier = pltpu.get_barrier_semaphore()
    sp_peer = [lax.rem(sp + k, n) for k in range(1, n)]
    tp_peer = [lax.rem(tp + k, tps) for k in range(1, tps)]
    dp_peer = [lax.rem(dp + k, dps) for k in range(1, dps)]
    place_peer = []
    for a in range(tps):
        for b in range(dps):
            if a or b:
                place_peer.append((lax.rem(tp + a, tps), lax.rem(dp + b, dps)))
    for p in sp_peer:
        pl.semaphore_signal(barrier, inc=1, device_id={"sp": p}, device_id_type=MESH)
    for a, b in place_peer:
        pl.semaphore_signal(barrier, inc=1, device_id={"tp": a, "dp": b}, device_id_type=MESH)
    sends = []

    def send(src, dst, ssem, rsem, dev):
        c = pltpu.make_async_remote_copy(
            src_ref=src, dst_ref=dst, send_sem=ssem, recv_sem=rsem,
            device_id=dev, device_id_type=MESH,
        )
        c.start()
        return c

    def arrived(dst, rsem):
        pltpu.make_async_copy(dst, dst, rsem).wait()

    for c in ld_conds:
        c.wait()
    act[...] = jnp.zeros(act.shape, F32)
    act[0:1, :] = silu(cond[...].astype(F32)).astype(BF16).astype(F32).reshape(1, -1)
    act[1:2, :] = silu(ctx_cond[...].astype(F32)).astype(BF16).astype(F32).reshape(1, -1)
    own_act = act[:, pl.ds(pl.multiple_of(sp * mod_rows, 128), mod_rows)].astype(BF16)
    ld_shift.wait()
    mod_part[0:2, :] = dot(own_act, mod_w[0])[0:2]
    ld_scale.wait()
    mod_part[2:4, :] = dot(own_act, mod_w[1])[0:2]
    ld_small = [load(src, dst) for src, dst in (
        (gain_h, gain), (sig_taps_h, sig_taps), (wr_taps_h, wr_taps), (rd_taps_h, rd_taps),
        (step_bias_h, step_bias), (decay_log_h, decay_log), (extra_h, extra), (group_gain_h, group_gain))]
    ld_lat = load(latent, lat_v.at[pl.ds(dp * half, half)])
    ld_ctx = load(context, ctx_v)
    ld_gatew = load(gate_w, mod_w.at[0])
    ld_sig = load(w_sig, w_all.at[:, pl.ds(sw, inner)])
    ld_wr = load(w_wr, w_all.at[:, pl.ds(0, sw)])
    ld_st = load(w_step, w_st)
    ld_rd = load(w_rd, w_all.at[:, pl.ds(inner + sw, sw)])
    ld_gate = load(w_gate, w_all.at[:, pl.ds(inner + 2 * sw, inner)])
    ld_outs = [
        load(w_out.at[pl.ds(q * inner + g * gw, gw)], w_o.at[g, pl.ds(q * gw, gw)])
        for g in range(group_count) for q in range(places)
    ]
    pl.semaphore_wait(barrier, len(sp_peer) + len(place_peer))
    for k, p in enumerate(sp_peer):
        sends.append(send(mod_part, mod_in.at[sp], mod_sem.at[0, k], mod_sem.at[1, sp], {"sp": p}))
    mod_in[sp] = mod_part[...]

    for k, p in enumerate(dp_peer):
        sends.append(send(latent, lat_v.at[pl.ds(dp * half, half)], lat_sem.at[0, k],
                          lat_sem.at[1, dp], {"dp": p}))

    def inv_rms(v):
        return lax.rsqrt(jnp.mean(v * v, axis=-1, keepdims=True) + EPSILON)

    lat_rms, ctx_rms = slice(0, 128), slice(128, 256)

    def row_tile(rows):
        return min(rows, 64)

    def rms_rows(ref, keep, start, count):
        tile = row_tile(count)

        def step(t, carry):
            at = pl.ds(pl.multiple_of(start + t * tile, tile), tile)
            total = jnp.zeros((tile, 128), F32)
            for c in range(width // 128):
                v = ref[at, c * 128:(c + 1) * 128].astype(F32)
                total = total + v * v
            mean = jnp.sum(total, axis=-1, keepdims=True) * (1.0 / width)
            in_block[at, keep] = jnp.broadcast_to(lax.rsqrt(mean + EPSILON), (tile, 128))
            return carry

        lax.fori_loop(0, count // tile, step, 0)

    ld_lat.wait()
    rms_rows(lat_v, lat_rms, dp * half, half)

    for p in sp_peer:
        arrived(mod_in.at[p], mod_sem.at[1, p])
    total = mod_in[0]
    for q in range(1, n):
        total = total + mod_in[q]
    mod_sum[...] = total
    for k, (a, b) in enumerate(place_peer):
        sends.append(send(mod_sum, mod_all.at[place], mod_sem.at[4, k], mod_sem.at[5, place],
                          {"tp": a, "dp": b}))
    mod_all[place] = total

    ld_ctx.wait()
    for p in dp_peer:
        arrived(lat_v.at[pl.ds(p * half, half)], lat_sem.at[1, p])
    pieces = width // 128
    first_lat = lat_v[0:16, :].astype(F32)[0:1]
    last_lat = lat_v[length - 16:length, :].astype(F32)[15:16]
    first_ctx = ctx_v[0:16, :].astype(F32)[0:1]
    last_ctx = ctx_v[ctx_len - 16:ctx_len, :].astype(F32)[15:16]
    for i in range(pieces):
        cols = slice(i * 128, (i + 1) * 128)
        edge_out[0, 0, i:i + 1, :] = last_lat[:, cols]
        edge_out[0, 1, i:i + 1, :] = last_ctx[:, cols]
        edge_out[1, 0, i:i + 1, :] = first_lat[:, cols]
        edge_out[1, 1, i:i + 1, :] = first_ctx[:, cols]

    def edge_copy(side):
        dev = sp + 1 if side == 0 else sp - 1
        return pltpu.make_async_remote_copy(
            src_ref=edge_out.at[side], dst_ref=edge_in.at[side], send_sem=edge_sem.at[0, side],
            recv_sem=edge_sem.at[1, side], device_id={"sp": dev}, device_id_type=MESH)

    @pl.when(sp < n - 1)
    def _():
        edge_copy(0).start()

    @pl.when(sp > 0)
    def _():
        edge_copy(1).start()

    for p in dp_peer:
        rms_rows(lat_v, lat_rms, p * half, half)
    rms_rows(ctx_v, ctx_rms, 0, ctx_len)
    own_out = pl.ds(pl.multiple_of(place * out_cols, 128), out_cols)

    def keep_rows(b, carry):
        at = pl.ds(pl.multiple_of(b * BLOCK, BLOCK), BLOCK)
        out[at, :] = lat_v[at, own_out]
        return carry

    lax.fori_loop(0, blocks, keep_rows, 0)
    ld_gatew.wait()
    gate_part[...] = dot(own_act, mod_w[0])[0:1]
    for k, p in enumerate(sp_peer):
        sends.append(send(gate_part, gate_in.at[sp], mod_sem.at[2, k], mod_sem.at[3, sp], {"sp": p}))
    gate_in[sp] = gate_part[...]

    low_r = lax.broadcasted_iota(jnp.int32, (BLOCK, BLOCK), 0)
    low_c = lax.broadcasted_iota(jnp.int32, (BLOCK, BLOCK), 1)
    lanes2 = 2 * heads
    er = lax.broadcasted_iota(jnp.int32, (lanes2, lanes2 * head_dim), 0)
    ec = lax.broadcasted_iota(jnp.int32, (lanes2, lanes2 * head_dim), 1)
    one = ((ec >= er * head_dim) & (ec < (er + 1) * head_dim)).astype(F32)
    spread[...] = jnp.concatenate([one, one, one], axis=0).astype(BF16)

    def widen(v):
        return jnp.concatenate(thirds(v), axis=1)

    for c in ld_small:
        c.wait()
    for a, b in place_peer:
        arrived(mod_all.at[a * dps + b], mod_sem.at[5, a * dps + b])
    for j in range(places):
        cols = slice(j * mod_cols, (j + 1) * mod_cols)
        block_mod = mod_all[j]
        g = gain[0:1, cols]
        for r in range(2):
            shift_rows[r, :, cols] = jnp.broadcast_to(block_mod[r:r + 1], (8, mod_cols))
            scale_rows[r, :, cols] = jnp.broadcast_to((1.0 + block_mod[2 + r:3 + r]) * g, (8, mod_cols))

    def hidden_rows(ref, keep, goal, which, start, count):
        tile = row_tile(count)

        def step(t, carry):
            at = pl.ds(pl.multiple_of(start + t * tile, tile), tile)
            r3 = in_block[at, keep].reshape(tile // 8, 8, 128)
            for c in range(width // 128):
                cols = slice(c * 128, (c + 1) * 128)
                v = ref[at, cols].astype(F32).reshape(tile // 8, 8, 128)
                h = v * r3 * scale_rows[which, :, cols][None] + shift_rows[which, :, cols][None]
                goal[at, cols] = h.reshape(tile, 128).astype(BF16)
            return carry

        lax.fori_loop(0, count // tile, step, 0)

    hidden_rows(ctx_v, ctx_rms, hid_c, 1, 0, ctx_len)

    @pl.when(sp > 0)
    def _():
        arrived(edge_in.at[0], edge_sem.at[1, 0])

    @pl.when(sp < n - 1)
    def _():
        arrived(edge_in.at[1], edge_sem.at[1, 1])

    edge_rows[...] = jnp.zeros(edge_rows.shape, F32)
    for i in range(pieces):
        cols = slice(i * 128, (i + 1) * 128)
        edge_rows[0:1, cols] = edge_in[0, 0, i:i + 1, :]
        edge_rows[1:2, cols] = edge_in[1, 0, i:i + 1, :]
        edge_rows[2:3, cols] = edge_in[0, 1, i:i + 1, :]
        edge_rows[3:4, cols] = edge_in[1, 1, i:i + 1, :]
    edge_v = edge_rows[...]
    edge_n = edge_v * inv_rms(edge_v)
    is_lat = lax.broadcasted_iota(jnp.int32, edge_v.shape, 0) < 2
    edge_hid = jnp.where(is_lat, edge_n * scale_rows[0] + shift_rows[0],
                         edge_n * scale_rows[1] + shift_rows[1])
    hid_c[ctx_len:ctx_len + 16, :] = jnp.concatenate([edge_hid, jnp.zeros_like(edge_hid)], axis=0).astype(BF16)

    ld_sig.wait()
    ld_wr.wait()
    ld_rd.wait()
    has_above = (sp > 0).astype(F32)
    has_below = (sp < n - 1).astype(F32)

    def ctx_proj(t, carry):
        cols = pl.ds(pl.multiple_of(t * TILE_N, TILE_N), TILE_N)
        got = dot(hid_c[...], w_all[:, cols]).astype(BF16).astype(F32)
        for i in range(TILE_N // 128):
            c, piece = t * (TILE_N // 128) + i, got[:, i * 128:(i + 1) * 128]
            raw_c[c, 8:8 + ctx_len, :] = piece[0:ctx_len]
            edges = piece[ctx_len:ctx_len + 8]
            raw[c, 0:8, :] = jnp.broadcast_to(edges[0:1] * has_above, (8, 128))
            raw[c, 8 + length:16 + length, :] = jnp.broadcast_to(edges[1:2] * has_below, (8, 128))
            raw_c[c, 0:8, :] = jnp.broadcast_to(edges[2:3] * has_above, (8, 128))
            raw_c[c, 8 + ctx_len:16 + ctx_len, :] = jnp.broadcast_to(edges[3:4] * has_below, (8, 128))
        return carry

    lax.fori_loop(0, (inner + 2 * sw) // TILE_N, ctx_proj, 0)
    ld_st.wait()
    ctx_step_in = dot_t(hid_c[0:ctx_len], w_st[...]).astype(BF16).astype(F32)

    bias = jnp.concatenate([step_bias[0:1], step_bias[1:2]], axis=1)
    rates = -jnp.exp(jnp.concatenate([decay_log[0:1], decay_log[1:2]], axis=1))

    def sums(ld, size):
        r = lax.broadcasted_iota(jnp.int32, (size, size), 0)
        c = lax.broadcasted_iota(jnp.int32, (size, size), 1)
        tri = jnp.concatenate([(r >= c).astype(F32), (r <= c).astype(F32)], axis=0).astype(BF16)
        parts = thirds(ld)
        both = dot(tri, parts[0]) + (dot(tri, parts[1]) + dot(tri, parts[2]))
        lane = lax.broadcasted_iota(jnp.int32, (1, ld.shape[1]), 1)
        forward = lax.rem(lane, lanes2) < heads
        cum = jnp.where(forward, both[:size], both[size:])
        return cum, jnp.where(forward, cum[size - 1:size], cum[0:1])

    def conv(ref, taps, first, start, count, cols, size):
        outs = []
        for i in range(count):
            tc = slice(cols + i * 128, cols + (i + 1) * 128)
            v = (taps[0:1, tc] * ref[first + i, pl.ds(start + 7, size), :]
                 + taps[1:2, tc] * ref[first + i, pl.ds(start + 8, size), :]
                 + taps[2:3, tc] * ref[first + i, pl.ds(start + 9, size), :])
            outs.append(silu(v))
        return outs[0] if count == 1 else jnp.concatenate(outs, axis=1)

    gp, sig_first, rd_first = gw // 128, sw // 128, (inner + sw) // 128

    def widened(v, cols):
        return dot(widen(v), spread[:, cols])

    def span_states(sig_g, wr_g, w_f, w_b):
        rhs = jnp.concatenate([sig_g * w_f, sig_g * w_b], axis=1).astype(BF16)
        return lax.dot_general(wr_g, rhs, (((0,), (0,)), ((), ())), preferred_element_type=F32)

    def group_cols(side, g):
        return slice(side * inner + g * gw, side * inner + (g + 1) * gw)

    ctx_step = softplus(ctx_step_in + bias)
    ctx_cum, ctx_end = sums(rates * ctx_step, ctx_len)
    ctx_w = widen(jnp.exp(ctx_end - ctx_cum) * ctx_step)
    ctx_dec8 = widened(jnp.broadcast_to(jnp.exp(ctx_end), (8, lanes2)), slice(0, 2 * inner))
    for g in range(group_count):
        sig_g = conv(raw_c, sig_taps, sig_first + g * gp, 0, gp, g * gw, ctx_len)
        wr_g = conv(raw_c, wr_taps, g, 0, 1, g * STATE, ctx_len).astype(BF16)
        got = span_states(sig_g, wr_g, dot(ctx_w, spread[:, group_cols(0, g)]),
                          dot(ctx_w, spread[:, group_cols(1, g)]))
        ctx_acc[0, g] = got[:, :gw]
        ctx_acc[1, g] = got[:, gw:]

    firsts = (0, n - 1)

    def ctx_copy(side, part):
        if part < group_count:
            src, dst = ctx_send.at[side, part], ctx_recv.at[side, sp, part]
        else:
            src, dst = cdec_send.at[side], cdec_recv.at[side, sp]
        return pltpu.make_async_remote_copy(
            src_ref=src, dst_ref=dst, send_sem=cchain_sem.at[0, side, 0, part],
            recv_sem=cchain_sem.at[1, side, sp, part], device_id={"sp": firsts[side]},
            device_id_type=MESH)

    for side in range(2):
        cdec_send[side] = ctx_dec8[0:1, side * inner:(side + 1) * inner]
        ctx_send[side] = ctx_acc[side].astype(BF16)
    for part in [group_count] + list(range(group_count)):
        for side in range(2):
            @pl.when(sp != firsts[side])
            def _():
                ctx_copy(side, part).start()

    def ctx_collect(side, g):
        for d in range(1, n):
            q = d if side == 0 else n - 1 - d
            if g == 0:
                arrived(cdec_recv.at[side, q], cchain_sem.at[1, side, q, group_count])
            arrived(ctx_recv.at[side, q, g], cchain_sem.at[1, side, q, g])
            ctx_acc[side, g] = (ctx_acc[side, g] * cdec_recv[side, q, :, g * gw:(g + 1) * gw]
                                + ctx_recv[side, q, g].astype(F32))

    hidden_rows(lat_v, lat_rms, lat_v, 0, 0, length)
    st_raw = dot_t(lat_v[...], w_st[...]).astype(BF16).astype(F32)

    def by_block(v):
        return jnp.concatenate([v] * blocks, axis=1)

    step = softplus(jnp.concatenate([st_raw[b * BLOCK:(b + 1) * BLOCK] for b in range(blocks)], axis=1)
                    + by_block(bias))
    more = jnp.concatenate([extra[:, b * BLOCK:(b + 1) * BLOCK] for b in range(blocks)], axis=0).T
    cum, end = sums(by_block(rates) * step + more, BLOCK)
    weight, grow = jnp.exp(end - cum) * step, jnp.exp(cum)
    cum_t, step_t = cum.T, step.T
    ends = jnp.exp(end)
    for b in range(blocks):
        at_b = slice(b * lanes2, (b + 1) * lanes2)
        cum_col[b] = cum[:, at_b]
        ecum_col[b] = widen(grow[:, at_b])
        weight_col[b] = widen(weight[:, at_b])
        cum_row[b] = cum_t[at_b]
        step_row[b] = step_t[at_b]
        dec[b] = widened(jnp.broadcast_to(ends[:, at_b], (8, lanes2)), slice(0, 2 * inner))
    dec_all = dec[0]
    for b in range(1, blocks):
        dec_all = dec_all * dec[b]
    for side in range(2):
        sdec_send[side] = dec_all[0:1, side * inner:(side + 1) * inner]

    def chain_copy(side, d, part):
        if part < group_count:
            src, dst = chain_out.at[side, part], chain_recv.at[side, sp, part]
        else:
            src, dst = sdec_send.at[side], sdec_recv.at[side, sp]
        return pltpu.make_async_remote_copy(
            src_ref=src, dst_ref=dst, send_sem=chain_sem.at[0, side, d, part],
            recv_sem=chain_sem.at[1, side, sp, part],
            device_id={"sp": sp + d if side == 0 else sp - d}, device_id_type=MESH)

    def has_goal(side, d):
        return sp + d < n if side == 0 else sp - d >= 0

    def is_source(side, q):
        return sp > q if side == 0 else sp < q

    for d in range(n - 1, 0, -1):
        for side in range(2):
            @pl.when(has_goal(side, d) & (sp != firsts[side]))
            def _():
                chain_copy(side, d, group_count).start()

    def chain_start(g):
        for side in range(2):
            @pl.when(sp == firsts[side])
            def _():
                ctx_collect(side, g)
                if n > 1:
                    chain_out[side, g] = (ctx_acc[side, g] * dec_all[0:1, group_cols(side, g)]
                                          + span_total[side, g]).astype(BF16)

            @pl.when(sp != firsts[side])
            def _():
                chain_out[side, g] = span_total[side, g].astype(BF16)
        for d in range(n - 1, 0, -1):
            for side in range(2):
                @pl.when(has_goal(side, d))
                def _():
                    chain_copy(side, d, g).start()

    def chain_end(g):
        for side in range(2):
            @pl.when(sp == firsts[side])
            def _():
                chain_in[side, g] = ctx_acc[side, g]

            if n > 1:
                @pl.when(sp != firsts[side])
                def _():
                    arrived(chain_recv.at[side, firsts[side], g], chain_sem.at[1, side, firsts[side], g])
                    chain_in[side, g] = chain_recv[side, firsts[side], g].astype(F32)

            for d in range(1, n - 1):
                q = d if side == 0 else n - 1 - d

                @pl.when(is_source(side, q))
                def _():
                    if g == 0:
                        arrived(sdec_recv.at[side, q], chain_sem.at[1, side, q, group_count])
                    arrived(chain_recv.at[side, q, g], chain_sem.at[1, side, q, g])
                    chain_in[side, g] = (
                        chain_in[side, g] * sdec_recv[side, q, :, g * gw:(g + 1) * gw]
                        + chain_recv[side, q, g].astype(F32))

    def hidden_dot(first, size):
        if size % 512 == 0:
            return dot(lat_v[...], w_all[:, first:first + size])
        near = dot(lat_v[:, :width // 2], w_all[:width // 2, first:first + size])
        return near + dot(lat_v[:, width // 2:], w_all[width // 2:, first:first + size])

    def project(first, size):
        got = hidden_dot(first, size).astype(BF16).astype(F32)
        for i in range(size // 128):
            raw[first // 128 + i, 8:8 + length, :] = got[:, i * 128:(i + 1) * 128]

    def gate_project(g):
        gates[:, g * gw:(g + 1) * gw] = hidden_dot(inner + 2 * sw + g * gw, gw).astype(BF16)

    def block_at(side, i):
        return i if side == 0 else blocks - 1 - i

    def side_cols(side):
        return slice(side * gw, (side + 1) * gw)

    def group_states(g):
        gc = slice(g * gw, (g + 1) * gw)

        def step(b, carry):
            start = pl.multiple_of(b * BLOCK, BLOCK)
            at = pl.ds(start, BLOCK)
            sig_g = conv(raw, sig_taps, sig_first + g * gp, start, gp, g * gw, BLOCK)
            wr_g = conv(raw, wr_taps, g, start, 1, g * STATE, BLOCK).astype(BF16)
            sig[at, gc] = sig_g.astype(BF16)
            wr[at, g * STATE:(g + 1) * STATE] = wr_g
            wide = weight_col[b]
            states[b, g] = span_states(sig_g, wr_g, dot(wide, spread[:, group_cols(0, g)]),
                                       dot(wide, spread[:, group_cols(1, g)]))
            return carry

        lax.fori_loop(0, blocks, step, 0, unroll=2)
        for side in range(2):
            def total_step(i, run):
                b = block_at(side, i)
                return run * dec[b, 0:1, group_cols(side, g)] + states[b, g, :, side_cols(side)]

            span_total[side, g] = lax.fori_loop(0, blocks, total_step, jnp.zeros((STATE, gw), F32))

    def group_blocks(g):
        gc = slice(g * gw, (g + 1) * gw)

        def step(b, carry):
            start = pl.multiple_of(b * BLOCK, BLOCK)
            at = pl.ds(start, BLOCK)
            cr, sr, cc = cum_row[b], step_row[b], cum_col[b]
            lane_g = lax.broadcasted_iota(jnp.int32, (BLOCK, gw), 1)
            rd_g = conv(raw, rd_taps, rd_first + g, start, 1, g * STATE, BLOCK).astype(BF16)
            rd[at, g * STATE:(g + 1) * STATE] = rd_g
            wr_g = wr[at, g * STATE:(g + 1) * STATE]
            sig_g = sig[at, gc]
            pair = dot_t(rd_g, wr_g)
            mixes, sigs = [], []
            for e in range(per_group):
                f, k = g * per_group + e, heads + g * per_group + e
                gap = jnp.where(low_r >= low_c, cc[:, f:f + 1] - cr[f:f + 1], cc[:, k:k + 1] - cr[k:k + 1])
                sf, sk = sr[f:f + 1], sr[k:k + 1]
                size = jnp.where(low_r > low_c, sf, jnp.where(low_r < low_c, sk, sf + sk))
                mixes.append((jnp.exp(gap) * size * pair).astype(BF16))
                mine = (lane_g >= e * head_dim) & (lane_g < (e + 1) * head_dim)
                sigs.append(jnp.where(mine, sig_g, jnp.zeros_like(sig_g)))
            in_block[at, gc] = dot(jnp.concatenate(mixes, axis=1), jnp.concatenate(sigs, axis=0))
            return carry

        lax.fori_loop(0, blocks, step, 0, unroll=2)

    chunk = pl.ds(pl.multiple_of(place * gw, 128), gw)

    def norm_copy(g, b, cols, dev, slot, sender):
        ref = normed.at[g, pl.ds(pl.multiple_of(b * BLOCK, BLOCK), BLOCK), cols]
        return pltpu.make_async_remote_copy(
            src_ref=ref, dst_ref=ref, send_sem=norm_sem.at[0, slot, g, b],
            recv_sem=norm_sem.at[1, sender, g, b], device_id=dev, device_id_type=MESH)

    def place_cols(q):
        return pl.ds(pl.multiple_of(q * gw, 128), gw)

    def finish_group(g):
        gc = slice(g * gw, (g + 1) * gw)
        for side in range(2):
            def enter(i, run):
                b = block_at(side, i)
                ent[b, g, :, side_cols(side)] = run.astype(BF16)
                return run * dec[b, 0:1, group_cols(side, g)] + states[b, g, :, side_cols(side)]

            lax.fori_loop(0, blocks, enter, chain_in[side, g])

        def finish(b, carry):
            at = pl.ds(pl.multiple_of(b * BLOCK, BLOCK), BLOCK)
            carried = dot(rd[at, g * STATE:(g + 1) * STATE], ent[b, g])
            grown = ecum_col[b]
            both = (in_block[at, gc]
                    + carried[:, :gw] * dot(grown, spread[:, group_cols(0, g)])
                    + carried[:, gw:] * dot(grown, spread[:, group_cols(1, g)]))
            gated = both * silu(gates[at, gc].astype(F32))
            done = gated * inv_rms(gated) * group_gain[0:1, gc]
            normed[g, at, chunk] = done.astype(BF16)
            for k, a in enumerate(tp_peer):
                norm_copy(g, b, chunk, {"tp": a}, k, place).start()
            for k, p in enumerate(dp_peer):
                norm_copy(g, b, chunk, {"dp": p}, tps - 1 + k, place).start()
            return carry

        lax.fori_loop(0, blocks, finish, 0)

    project(0, sw + gw)
    group_states(0)
    chain_start(0)
    for g in range(1, group_count):
        project(sw + g * gw, gw)
        group_states(g)
    project(sw + inner, sw)
    for g in range(1, group_count):
        chain_start(g)
    ld_gate.wait()
    for g in range(group_count):
        group_blocks(g)
        gate_project(g)
        chain_end(g)
        finish_group(g)

    for p in sp_peer:
        arrived(gate_in.at[p], mod_sem.at[3, p])
    gate_vec = gate_in[0]
    for q in range(1, n):
        gate_vec = gate_vec + gate_in[q]

    for c in ld_outs:
        c.wait()
    slots = (tps - 1) + (dps - 1)

    def relay(g, b):
        for k, a in enumerate(tp_peer):
            q = a * dps + dp
            norm_copy(g, b, place_cols(q), {"tp": a}, 0, q).wait_recv()
            for j, p in enumerate(dp_peer):
                slot = slots + k * (dps - 1) + j
                norm_copy(g, b, place_cols(q), {"dp": p}, slot, q).start()

    def gathered(g, b):
        for p in dp_peer:
            for a in range(tps):
                q = a * dps + p
                norm_copy(g, b, place_cols(q), {"dp": p}, 0, q).wait_recv()

    def held(b):
        return jnp.concatenate([states[b, j] for j in range(group_count)], axis=1)

    for g in range(group_count - 1):
        lax.fori_loop(0, blocks, lambda b, carry: (relay(g, b), carry)[1], 0)
        lax.fori_loop(0, blocks, lambda b, carry: (gathered(g, b), carry)[1], 0)
        part = dot(normed[g], w_o[g])
        for b in range(blocks):
            piece = part[b * BLOCK:(b + 1) * BLOCK]
            if g > 0:
                piece = piece + held(b)
            for j in range(group_count):
                states[b, j] = piece[:, j * 2 * gw:(j + 1) * 2 * gw]

    def finished(first, count):
        g = group_count - 1
        for b in range(first, first + count):
            gathered(g, b)
        at = pl.ds(first * BLOCK, count * BLOCK)
        part = dot(normed[g, at, :], w_o[g])
        if g > 0:
            part = part + jnp.concatenate([held(b) for b in range(first, first + count)], axis=0)
        out[at, :] = (out[at, :].astype(F32) + gate_vec * part).astype(BF16)

    spans, first = [], 0
    while first < blocks:
        count = 2 if blocks - first > 2 else 1
        spans.append((first, count))
        first += count
    for i, (first, count) in enumerate(spans):
        for b in range(first, first + count):
            relay(group_count - 1, b)
        if i > 0:
            finished(*spans[i - 1])
    finished(*spans[-1])

    for c in sends:
        c.wait_send()

    @pl.when(sp < n - 1)
    def _():
        edge_copy(0).wait_send()

    @pl.when(sp > 0)
    def _():
        edge_copy(1).wait_send()

    for side in range(2):
        @pl.when(sp != firsts[side])
        def _():
            for part in range(group_count + 1):
                ctx_copy(side, part).wait_send()

        for d in range(1, n):
            @pl.when(has_goal(side, d))
            def _():
                for g in range(group_count):
                    chain_copy(side, d, g).wait_send()

            @pl.when(has_goal(side, d) & (sp != firsts[side]))
            def _():
                chain_copy(side, d, group_count).wait_send()

    for g in range(group_count):
        def drained(b, carry):
            for k, a in enumerate(tp_peer):
                norm_copy(g, b, chunk, {"tp": a}, k, place).wait_send()
            for k, p in enumerate(dp_peer):
                norm_copy(g, b, chunk, {"dp": p}, tps - 1 + k, place).wait_send()
            for k, a in enumerate(tp_peer):
                for j, p in enumerate(dp_peer):
                    slot = slots + k * (dps - 1) + j
                    norm_copy(g, b, place_cols(a * dps + dp), {"dp": p}, slot, place).wait_send()
            return carry

        lax.fori_loop(0, blocks, drained, 0)


def on_device(dims, *args):
    (
        latent, context, condition, context_condition, shift_weight, scale_weight, gate_weight,
        norm_gain, out_gate_weight, signal_weight, writer_weight, reader_matrix, step_weight,
        signal_taps, writer_taps, reader_taps, step_bias, decay_log, decay_extra, group_gain,
        output_weight,
    ) = args
    n, tps, dps = dims
    half, width = latent.shape
    length = half * dps
    ctx_len = context.shape[0]
    heads = step_bias.shape[1]
    inner = signal_weight.shape[1]
    sw = writer_weight.shape[1]
    groups = sw // STATE
    gw = inner // groups
    blocks = length // BLOCK
    places = tps * dps
    mod_rows, mod_cols = shift_weight.shape
    out_cols = output_weight.shape[1]
    lanes2 = 2 * heads
    conv_cols = inner + 2 * sw
    steps = jnp.swapaxes(step_weight, 1, 2).reshape(lanes2, width)
    hbm = pl.BlockSpec(memory_space=pltpu.HBM)
    vmem = pl.BlockSpec(memory_space=pltpu.VMEM)
    slots = (tps - 1) + (dps - 1) + (tps - 1) * (dps - 1)
    peers = max(n - 1, places - 1, 1)
    small = (condition, context_condition, norm_gain.reshape(1, -1), signal_taps, writer_taps,
             reader_taps, step_bias, decay_log, decay_extra.reshape(lanes2, length),
             group_gain.reshape(1, -1))
    scratch = [pltpu.VMEM(v.shape, v.dtype) for v in small] + [
        pltpu.VMEM((length, width), BF16),
        pltpu.VMEM((ctx_len, width), BF16),
        pltpu.VMEM((8, width), F32),
        pltpu.VMEM((2, mod_rows, mod_cols), BF16),
        pltpu.VMEM((4, mod_cols), F32),
        pltpu.VMEM((1, mod_cols), F32),
        pltpu.VMEM((n, 4, mod_cols), F32),
        pltpu.VMEM((n, 1, mod_cols), F32),
        pltpu.VMEM((4, mod_cols), F32),
        pltpu.VMEM((places, 4, mod_cols), F32),
        pltpu.VMEM((2, 8, width), F32),
        pltpu.VMEM((2, 8, width), F32),
        pltpu.VMEM((2, 2, width // 128, 128), F32),
        pltpu.VMEM((2, 2, width // 128, 128), F32),
        pltpu.VMEM((8, width), F32),
        pltpu.VMEM((ctx_len + 16, width), BF16),
        pltpu.VMEM((width, 2 * inner + 2 * sw), BF16),
        pltpu.VMEM((lanes2, width), BF16),
        pltpu.VMEM((groups, places * gw, out_cols), BF16),
        pltpu.VMEM((conv_cols // 128, length + 16, 128), F32),
        pltpu.VMEM((conv_cols // 128, ctx_len + 16, 128), F32),
        pltpu.VMEM((length, inner), BF16),
        pltpu.VMEM((blocks, BLOCK, lanes2), F32),
        pltpu.VMEM((blocks, BLOCK, 3 * lanes2), BF16),
        pltpu.VMEM((blocks, BLOCK, 3 * lanes2), BF16),
        pltpu.VMEM((blocks, lanes2, BLOCK), F32),
        pltpu.VMEM((blocks, lanes2, BLOCK), F32),
        pltpu.VMEM((length, inner), BF16),
        pltpu.VMEM((length, sw), BF16),
        pltpu.VMEM((length, sw), BF16),
        pltpu.VMEM((blocks, groups, STATE, 2 * gw), F32),
        pltpu.VMEM((blocks, 8, 2 * inner), F32),
        pltpu.VMEM((blocks, groups, STATE, 2 * gw), BF16),
        pltpu.VMEM((2, groups, STATE, gw), F32),
        pltpu.VMEM((2, groups, STATE, gw), BF16),
        pltpu.VMEM((2, n, groups, STATE, gw), BF16),
        pltpu.VMEM((2, 1, inner), F32),
        pltpu.VMEM((2, n, 1, inner), F32),
        pltpu.VMEM((2, 1, inner), F32),
        pltpu.VMEM((2, n, 1, inner), F32),
        pltpu.VMEM((2, groups, STATE, gw), F32),
        pltpu.VMEM((2, groups, STATE, gw), BF16),
        pltpu.VMEM((2, n, groups, STATE, gw), BF16),
        pltpu.VMEM((2, groups, STATE, gw), F32),
        pltpu.VMEM((3 * lanes2, 2 * inner), BF16),
        pltpu.VMEM((length, inner), F32),
        pltpu.VMEM((groups, length, places * gw), BF16),
        pltpu.SemaphoreType.DMA((20 + groups * places,)),
        pltpu.SemaphoreType.DMA((2, dps)),
        pltpu.SemaphoreType.DMA((6, max(n, places))),
        pltpu.SemaphoreType.DMA((2, 2)),
        pltpu.SemaphoreType.DMA((2, 2, n, groups + 1)),
        pltpu.SemaphoreType.DMA((2, 2, n, groups + 1)),
        pltpu.SemaphoreType.DMA((2, max(slots, places), groups, blocks)),
    ]
    specs = [hbm] * 21
    operands = (
        latent, context, condition, context_condition, shift_weight, scale_weight, gate_weight,
        norm_gain.reshape(1, -1), out_gate_weight, signal_weight, writer_weight, reader_matrix,
        steps, signal_taps, writer_taps, reader_taps, step_bias, decay_log,
        decay_extra.reshape(lanes2, length), group_gain.reshape(1, -1), output_weight,
    )
    return pl.pallas_call(
        functools.partial(kernel, dims),
        out_shape=pltpu.VMEM((length, out_cols), BF16),
        in_specs=specs,
        out_specs=vmem,
        scratch_shapes=scratch,
        compiler_params=pltpu.CompilerParams(
            collective_id=0, has_side_effects=True, vmem_limit_bytes=60000000),
    )(*[pltpu.with_memory_space_constraint(x, pltpu.HBM) for x in operands])


def solution(mesh):
    dims = (mesh.shape["sp"], mesh.shape["tp"], mesh.shape["dp"])
    in_specs = (
        P(("grp", "sp", "dp"), None),
        P(("grp", "sp"), None),
        P("grp"),
        P(),
        P("sp", ("tp", "dp")),
        P("sp", ("tp", "dp")),
        P("sp", ("tp", "dp")),
        P(),
        P(None, ("tp", "dp")),
        P(None, ("tp", "dp")),
        P(None, ("tp", "dp")),
        P(None, ("tp", "dp")),
        P(None, None, ("tp", "dp")),
        P(None, ("tp", "dp")),
        P(None, ("tp", "dp")),
        P(None, ("tp", "dp")),
        P(None, ("tp", "dp")),
        P(None, ("tp", "dp")),
        P(None, ("tp", "dp"), ("grp", "sp")),
        P(("tp", "dp")),
        P(None, ("tp", "dp")),
    )
    out_specs = P(("grp", "sp"), ("tp", "dp"))
    return jax.shard_map(
        functools.partial(on_device, dims), mesh=mesh, in_specs=in_specs, out_specs=out_specs,
        check_vma=False,
    )
```
